256 devices in a mesh: sp: 64 (over z, y, core), tp: 4 (over x).
Axes of the slice: x: 4, y: 4, z: 8, core: 2. Of those that a mesh axis runs over, the one named last changes fastest.
Arguments:
- residual: bfloat16 [16384, 2048], P(('sp', 'tp')), may hold values from -6 to 6
- queries: bfloat16 [16384, 2048], P('sp', 'tp'), may hold values from -40 to 40
- key_rows: bfloat16 [16384, 1024], P('sp', 'tp'), may hold values from -40 to 40
- value_rows: bfloat16 [16384, 1024], P('sp', 'tp'), may hold values from -6 to 6
- forget_sums: float32 [16384, 16], P('sp', 'tp'), as said below
- out_weight: bfloat16 [2048, 2048], P('tp'), may hold values from -0.25 to 0.25
- norm_gain: float32 [2048], replicated, may hold values from 0.1 to 1.9
- expert_ids: int32 [16384, 4], P(('sp', 'tp')), may hold values from 0 to 63, all different within a row; in each aligned block of 64 rows (0 to 63, 64 to 127, ...) at most 8 rows name the same one
- route_weights: float32 [16384, 4], P(('sp', 'tp')), may hold values from 0.1 to 1
- expert_gate: bfloat16 [64, 2048, 384], P('sp'), may hold values from -0.125 to 0.125
- expert_up: bfloat16 [64, 2048, 384], P('sp'), may hold values from -0.125 to 0.125
- expert_down: bfloat16 [64, 384, 2048], P('sp'), may hold values from -0.3125 to 0.3125
- shared_gate: bfloat16 [2048, 384], replicated, may hold values from -0.125 to 0.125
- shared_up: bfloat16 [2048, 384], replicated, may hold values from -0.125 to 0.125
- shared_down: bfloat16 [384, 2048], replicated, may hold values from -0.3125 to 0.3125
Outputs:
- layer_out: bfloat16 [16384, 2048], P(('sp', 'tp'))
The draws below stay inside these ranges and needn't reach their ends.
Inputs may be any that keep to these rules, and one draw needn't show every extreme that they name: `forget_sums`: each head's column never rises from one position to the next. `expert_ids`: each row names 4 different experts; among the rows of one device no expert is named more than 8 times.
All inputs are finite; a program needn't handle non-finite values.
Results may differ from the reference program's by a relative error of at most 0.014.
Values may be sent and summed in bfloat16 or wider, within the bound.
No kernel may reach another device: no remote copies, remote signals or barrier semaphores. Data moves between devices by JAX's collectives and lax.ppermute only.
A program may use at most 128 MiB of HBM per device.

```python
import math
import jax
import jax.numpy as jnp
import numpy as np
from jax import lax

D = 2048
HEADS = 16
KV_HEADS = 8
HEAD_DIM = 128
FE = 384
FS = 384
TOPK = 4
TOK_DEV = 256
EXPERTS = 64
TOKENS = 16384
ROWS = 64
CAP = 8


def query_key_pair(key):
    base_seed = jax.random.fold_in(key, 11)
    seed_list = jax.random.split(base_seed, 2)
    query_rows = 1.3 * jax.random.normal(seed_list[0], (TOKENS, HEADS * HEAD_DIM), jnp.float32)
    key_block = 1.3 * jax.random.normal(seed_list[1], (TOKENS, KV_HEADS * HEAD_DIM), jnp.float32)
    return (jnp.clip(query_rows, -40.0, 40.0), jnp.clip(key_block, -40.0, 40.0))


def draw_queries(key, part):
    return query_key_pair(key)[0].astype(jnp.bfloat16)


def draw_key_rows(key, part):
    return query_key_pair(key)[1].astype(jnp.bfloat16)


def draw_forget_sums(key, part):
    base_seed = jax.random.fold_in(key, 23)
    seed_list = jax.random.split(base_seed, 7)
    ordering = jax.random.permutation(seed_list[0], HEADS)
    slowly = ordering < HEADS // 2
    slow_rate = jax.random.uniform(seed_list[1], (HEADS,), jnp.float32, 0.25, 1.0) / TOKENS
    fast_rate = jnp.exp(jax.random.uniform(seed_list[2], (HEADS,), jnp.float32, math.log(0.01), math.log(1.0 / 30.0)))
    rates = jnp.where(slowly, slow_rate, fast_rate)
    block_count = TOKENS // TOK_DEV
    factor = jnp.exp(jax.random.uniform(seed_list[3], (block_count, 1), jnp.float32, -0.7, 0.7))
    factor = jnp.repeat(factor, TOK_DEV, axis=0)
    rough = jax.random.uniform(seed_list[4], (TOKENS, HEADS), jnp.float32, 0.2, 1.8)
    log_steps = -rates[None, :] * factor * rough
    places = jax.random.randint(seed_list[5], (3,), 0, TOKENS)
    losses = jnp.log(jax.random.uniform(seed_list[6], (3, HEADS), jnp.float32, 0.5, 0.8))
    log_steps = log_steps.at[places].add(jnp.where(slowly[None, :], losses, 0.0))
    return jnp.cumsum(log_steps, axis=0)


def block_levels(rng, dims, pieces, smallest, high):
    factor_of, own = 1.0, jax.random.fold_in(rng, 6)
    for dim, parts in pieces:
        heights = jnp.exp(jax.random.uniform(jax.random.fold_in(own, dim), (parts,), jnp.float32, smallest / len(pieces), high / len(pieces)))
        factor_of = factor_of * jnp.repeat(heights, dims[dim] // parts).reshape([-1 if axis == dim else 1 for axis in range(len(dims))])
    return factor_of


def assign_block(own_key, own, number, rows, count, top, most, skew):
    sequence = jax.random.permutation(own_key, count)
    crowded, common = load_shares(count, rows * top, most, skew, True), load_shares(count, rows * top, most, skew, False)
    places = jnp.arange(count)

    def named(lengths, rotation):
        used = int((lengths > 0).sum())
        fixed = max(1, used // 4)
        moved = fixed + (places - fixed + rotation * (used - fixed)) % max(1, count - fixed)
        return jnp.zeros((count,), jnp.int32).at[sequence[jnp.where(places < fixed, places, moved)]].set(jnp.asarray(lengths, jnp.int32))

    lengths = jnp.where(number % 4 == 0, named(crowded, number // 4), named(common, number - number // 4 - 1))
    mixed = jax.random.permutation(jax.random.fold_in(own, 3), count)
    source_of, receiver = mixed[0:count // 2 * 2:2], mixed[1:count // 2 * 2:2]
    margin = jnp.minimum(lengths[source_of] - 1, most - lengths[receiver]) // 2
    margin = jnp.where((source_of == sequence[0]) | (receiver == sequence[0]) | (lengths[receiver] == 0), 0, jnp.maximum(margin, 0))
    moved = jax.random.randint(jax.random.fold_in(own, 4), (count // 2,), 0, 1 << 20) % (margin + 1)
    lengths = lengths.at[source_of].add(-moved).at[receiver].add(moved)
    labels = jnp.searchsorted(jnp.cumsum(lengths), jnp.arange(rows * top), side="right").astype(jnp.int32)
    grid = labels.reshape(top, rows).T
    grid = grid[jax.random.permutation(jax.random.fold_in(own, 1), rows)]
    rotation = jax.random.randint(jax.random.fold_in(own, 2), (rows, 1), 0, top)
    return jnp.take_along_axis(grid, (jnp.arange(top)[None, :] + rotation) % top, axis=1)


def load_shares(count, total, reach, lean, full):
    weights = [(1 << 20) // math.isqrt(grade ** lean) + 1 for grade in range(1, count + 1)]
    largest = reach if full else min(reach, max(-(-total // count), total * weights[0] // sum(weights)))
    least = 1 if total - largest >= count - 1 else 0
    given, surplus = [largest] + [least] * (count - 1), total - largest - least * (count - 1)
    while surplus > 0:
        free = [i for i in range(1, count) if given[i] < largest] or [i for i in range(1, count) if given[i] < reach]
        whole, budget = sum([weights[i] for i in free]), surplus
        for i in free:
            more = min(reach - given[i], max(1, budget * weights[i] // whole), surplus)
            given[i] = given[i] + more
            surplus = surplus - more
    return np.array(given)


def scatter_about(own_key, extent, scale, limit, cuts=(), held_as=jnp.bfloat16):
    values = scale * jax.random.normal(own_key, extent, jnp.float32)
    if cuts:
        values = values * block_levels(own_key, extent, cuts, -0.22, 0.18)
    return jnp.clip(values, -limit, limit).astype(held_as)


def setup_inputs(seed: int = 0) -> dict:
    splits = jax.random.split(jax.random.key(seed), 16)
    residual = scatter_about(splits[0], (TOKENS, D), 1.0, 6.0, ((0, 256),))
    queries = draw_queries(jax.random.fold_in(splits[15], 71), 0)
    key_rows = draw_key_rows(jax.random.fold_in(splits[15], 71), 0)
    value_rows = scatter_about(splits[3], (TOKENS, KV_HEADS * HEAD_DIM), 1.0, 6.0, ((0, 64), (1, 4)))
    forget_sums = draw_forget_sums(jax.random.fold_in(splits[15], 71), 0)
    out_weight = scatter_about(splits[5], (HEADS * HEAD_DIM, D), (HEADS * HEAD_DIM // 4) ** -0.5, 0.25, ((0, 4),))
    norm_gain = jnp.clip(1.0 + 0.18 * jax.random.normal(splits[6], (D,), jnp.float32), 0.1, 1.9)
    expert_ids_keys = jax.random.split(jax.random.fold_in(splits[7], 1), TOKENS // ROWS)
    expert_ids_turns = jax.random.permutation(jax.random.fold_in(splits[7], 3), TOKENS // ROWS)
    expert_ids = jax.vmap(lambda own, number: assign_block(jax.random.fold_in(splits[7], 2), own, number, ROWS, EXPERTS, TOPK, CAP, 2))(expert_ids_keys, expert_ids_turns).reshape((TOKENS, TOPK))
    route_weights = jnp.clip(jnp.exp(math.log(1.0) - 2.3025851 * jax.random.uniform(splits[8], (TOKENS, TOPK), jnp.float32) ** block_levels(splits[8], (TOKENS, TOPK), ((0, 256),), -0.2, 0.2)), 0.1, 1.0)
    expert_gate = scatter_about(splits[9], (EXPERTS, D, FE), D ** -0.5, 0.125, ((0, 64),))
    expert_up = scatter_about(splits[10], (EXPERTS, D, FE), D ** -0.5, 0.125, ((0, 64),))
    expert_down = scatter_about(splits[11], (EXPERTS, FE, D), FE ** -0.5, 0.3125, ((0, 64),))
    shared_gate = scatter_about(splits[12], (D, FS), D ** -0.5, 0.125)
    shared_up = scatter_about(splits[13], (D, FS), D ** -0.5, 0.125)
    shared_down = scatter_about(splits[14], (FS, D), FS ** -0.5, 0.3125)
    return {"residual": residual, "queries": queries, "key_rows": key_rows, "value_rows": value_rows, "forget_sums": forget_sums, "out_weight": out_weight, "norm_gain": norm_gain, "expert_ids": expert_ids, "route_weights": route_weights, "expert_gate": expert_gate, "expert_up": expert_up, "expert_down": expert_down, "shared_gate": shared_gate, "shared_up": shared_up, "shared_down": shared_down}


routed_scale = 2.5
norm_eps = 1e-06

def attend(queries, key_rows, value_rows, forget_sums):
    group_size = HEADS // KV_HEADS
    score_scale = HEAD_DIM ** (-0.5)
    key_heads = key_rows.astype(jnp.float32).reshape(TOKENS, KV_HEADS, HEAD_DIM)
    value_heads = value_rows.astype(jnp.float32).reshape(TOKENS, KV_HEADS, HEAD_DIM)
    key_sums = forget_sums.reshape(TOKENS, KV_HEADS, group_size).transpose(1, 2, 0)
    positions = jnp.arange(TOKENS, dtype=jnp.int32)
    block_rows = math.gcd(TOKENS, 256)

    def one_block(first_pos):
        query_block = lax.dynamic_slice_in_dim(queries, first_pos, block_rows, 0).astype(jnp.float32)
        query_block = query_block.reshape(block_rows, KV_HEADS, group_size, HEAD_DIM)
        query_sums = lax.dynamic_slice_in_dim(forget_sums, first_pos, block_rows, 0)
        query_sums = query_sums.reshape(block_rows, KV_HEADS, group_size).transpose(1, 2, 0)
        scores = jnp.einsum('qhgd,khd->hgqk', query_block, key_heads) * score_scale
        scores = scores + (query_sums[:, :, :, None] - key_sums[:, :, None, :])
        query_pos = first_pos + jnp.arange(block_rows, dtype=jnp.int32)
        allowed = query_pos[:, None] >= positions[None, :]
        scores = jnp.where(allowed, scores, -jnp.inf)
        row_max = lax.optimization_barrier(jnp.max(scores, axis=3, keepdims=True))
        weights = jnp.exp(scores - row_max)
        weight_sum = lax.optimization_barrier(jnp.sum(weights, axis=3))
        rounded = lax.optimization_barrier(weights.astype(jnp.bfloat16)).astype(jnp.float32)
        mixed = jnp.einsum('hgqk,khd->qhgd', rounded, value_heads)
        mixed = mixed / weight_sum.transpose(2, 0, 1)[:, :, :, None]
        return mixed.reshape(block_rows, HEADS * HEAD_DIM).astype(jnp.bfloat16)
    starts = jnp.arange(TOKENS // block_rows, dtype=jnp.int32) * block_rows
    return lax.map(one_block, starts).reshape(TOKENS, HEADS * HEAD_DIM)

def experts_all(normed, expert_ids, route_weights, expert_gate, expert_up, expert_down):
    slot_count = TOKENS // ROWS * CAP
    flat_ids = expert_ids.reshape(-1)
    assigned = flat_ids.shape[0]
    gates = route_weights / lax.optimization_barrier(jnp.sum(route_weights, axis=1, keepdims=True)) * routed_scale
    flat_gates = jnp.concatenate([gates.reshape(-1), jnp.zeros((1,), jnp.float32)])
    padded = jnp.concatenate([normed, jnp.zeros((1, D), jnp.bfloat16)])

    def one_expert(carried, expert):
        chosen = flat_ids == expert
        place = jnp.where(chosen, jnp.cumsum(chosen.astype(jnp.int32)) - 1, slot_count)
        source = jnp.full((slot_count + 1,), assigned, jnp.int32)
        source = source.at[place].set(jnp.arange(assigned, dtype=jnp.int32))[:slot_count]
        token_rows = padded[source // TOPK]
        gate_part = jnp.dot(token_rows, expert_gate[expert], preferred_element_type=jnp.float32)
        up_part = jnp.dot(token_rows, expert_up[expert], preferred_element_type=jnp.float32)
        hidden = (jax.nn.silu(gate_part) * up_part).astype(jnp.bfloat16)
        output = jnp.dot(hidden, expert_down[expert], preferred_element_type=jnp.float32).astype(jnp.bfloat16)
        carried = carried.at[source // TOPK].add(flat_gates[source][:, None] * output.astype(jnp.float32))
        return (carried, None)
    routed, _ = lax.scan(one_expert, jnp.zeros((TOKENS + 1, D), jnp.float32), jnp.arange(EXPERTS, dtype=jnp.int32))
    return routed[:TOKENS]

def reference(residual, queries, key_rows, value_rows, forget_sums, out_weight, norm_gain, expert_ids, route_weights, expert_gate, expert_up, expert_down, shared_gate, shared_up, shared_down):
    attended = attend(queries, key_rows, value_rows, forget_sums)
    branch = jnp.dot(attended, out_weight, preferred_element_type=jnp.float32)
    stream = (residual.astype(jnp.float32) + branch).astype(jnp.bfloat16)
    wide = lax.optimization_barrier(stream).astype(jnp.float32)
    normed = (wide * lax.rsqrt(lax.optimization_barrier(jnp.mean(wide * wide, axis=1, keepdims=True)) + norm_eps) * norm_gain).astype(jnp.bfloat16)
    routed = experts_all(normed, expert_ids, route_weights, expert_gate, expert_up, expert_down)
    shared_hidden = (jax.nn.silu(jnp.dot(normed, shared_gate, preferred_element_type=jnp.float32)) * jnp.dot(normed, shared_up, preferred_element_type=jnp.float32)).astype(jnp.bfloat16)
    shared_out = jnp.dot(shared_hidden, shared_down, preferred_element_type=jnp.float32)
    return (wide + shared_out + routed).astype(jnp.bfloat16)
```

```python
import functools
import math

import jax
import jax.numpy as jnp
from jax import lax
from jax.experimental import pallas as pl
from jax.experimental.pallas import tpu as pltpu
from jax.sharding import Mesh, PartitionSpec as P

HEADS = 16
KV_HEADS = 8
HEAD_DIM = 128
TOPK = 4
ROUTED_SCALE = 2.5
NORM_EPS = 1e-06
LOG2E = math.log2(math.e)
SCORE2 = HEAD_DIM**-0.5 * LOG2E
LOW = -1e30
TAIL = 16

BF = jnp.bfloat16
F32 = jnp.float32


def pieces(row):
    high = row.astype(BF)
    rest = row - high.astype(F32)
    mid = rest.astype(BF)
    low = (rest - mid.astype(F32)).astype(BF)
    return [high.astype(F32), mid.astype(F32), low.astype(F32)]


def tail_block(rows, width):
    parts = [piece for row in rows for piece in pieces(row)]
    parts.append(jnp.zeros((TAIL - len(parts), width), F32))
    return jnp.concatenate(parts, axis=0).astype(BF)


def row_of(tail, j):
    return tail[3 * j : 3 * j + 1] + tail[3 * j + 1 : 3 * j + 2] + tail[3 * j + 2 : 3 * j + 3]


def pack_kernel(q_ref, k_ref, v_ref, f_ref, kv_out, q_out):
    rows = q_ref.shape[0]
    ys = q_out.shape[0] // 2
    for c in range(2):
        tail = tail_block([f_ref[2 * c : 2 * c + 1, :], f_ref[2 * c + 1 : 2 * c + 2, :]], rows)
        kv_out[c, :rows, :HEAD_DIM] = k_ref[:, c * HEAD_DIM : (c + 1) * HEAD_DIM]
        kv_out[c, :rows, HEAD_DIM:] = v_ref[:, c * HEAD_DIM : (c + 1) * HEAD_DIM]
        kv_out[c, rows:, :] = tail
        q_part = q_ref[:, c * 2 * HEAD_DIM : (c + 1) * 2 * HEAD_DIM]
        for y in range(ys):
            q_out[2 * y + c, :rows, :] = q_part
            q_out[2 * y + c, rows:, :] = tail


def pack(q, k, v, f_t, ys):
    rows = q.shape[0]
    width = 2 * HEAD_DIM
    return pl.pallas_call(
        pack_kernel,
        out_shape=(
            jax.ShapeDtypeStruct((2, rows + TAIL, width), BF),
            jax.ShapeDtypeStruct((2 * ys, rows + TAIL, width), BF),
        ),
        name="pack",
    )(q, k, v, f_t)


def attend_kernel(info, *refs, blocks, own, first, last, tiles, rows):
    q_ref, ref_tail = refs[0], refs[1]
    kv_refs = refs[2 : 2 + blocks]
    at = 2 + blocks
    if not first:
        acc_in, stat_in = refs[at], refs[at + 1]
        at += 2
    if last:
        (o_out,) = refs[at : at + 1]
    else:
        acc_out, stat_out = refs[at : at + 2]
    step = pl.program_id(0)
    first_tail = ref_tail[0].astype(F32)
    keys, values, biases = [], [], []
    ones = jnp.ones((rows, HEAD_DIM), BF)
    for b in range(blocks):
        for c in range(2):
            keys.append(kv_refs[b].at[c, pl.ds(0, rows), pl.ds(0, HEAD_DIM)])
            values.append(kv_refs[b].at[c, pl.ds(0, rows), pl.ds(HEAD_DIM, HEAD_DIM)])
            tail = kv_refs[b][c, rows:, :].astype(F32)
            pair = []
            for j in range(2):
                bias = (row_of(first_tail, j)[:, :1] - row_of(tail, j)) * LOG2E
                pair.append(jnp.where(info[1 + b] > 0, bias, -jnp.inf))
            biases.append(pair)
    lane = lax.broadcasted_iota(jnp.int32, (rows, HEAD_DIM), 1)
    for i in range(tiles):
        tile_first = (step * tiles + i) * rows
        if not first:
            stat_old = stat_in[i]
        stat_new = jnp.zeros((rows, HEAD_DIM), F32)
        lse_rows = []
        for j in range(2):
            cols = pl.ds(j * HEAD_DIM, HEAD_DIM)
            query = q_ref[i, pl.ds(0, rows), cols]
            scores = []
            for u in range(2 * blocks):
                raw = lax.dot_general(
                    query, keys[u][...], (((1,), (1,)), ((), ())), preferred_element_type=F32
                )
                score = raw * SCORE2 + biases[u][j]
                if own and u < 2:
                    q_pos = tile_first + lax.broadcasted_iota(jnp.int32, (rows, rows), 0)
                    k_pos = info[0] + u * rows + lax.broadcasted_iota(jnp.int32, (rows, rows), 1)
                    score = jnp.where(q_pos >= k_pos, score, -jnp.inf)
                scores.append(score)
            top = scores[0]
            for score in scores[1:]:
                top = jnp.maximum(top, score)
            row_max = jnp.max(top, axis=1, keepdims=True)
            if first:
                row_max = jnp.maximum(row_max, LOW)
            else:
                old_max = stat_old[:, j : j + 1]
                row_max = jnp.maximum(row_max, old_max)
            total = None
            for u in range(2 * blocks):
                weights = jnp.exp2(scores[u] - row_max).astype(BF)
                value = jnp.concatenate([values[u][...], ones], axis=1)
                part = jnp.dot(weights, value, preferred_element_type=F32)
                total = part if total is None else total + part
            weighted = total[:, :HEAD_DIM]
            row_sum = total[:, HEAD_DIM : HEAD_DIM + 1]
            if not first:
                factor = jnp.exp2(old_max - row_max)
                weighted = weighted + acc_in[i, :, cols] * factor
                row_sum = row_sum + stat_old[:, 2 + j : 3 + j] * factor
            if last:
                some = row_sum > 0.0
                mixed = weighted * (1.0 / jnp.where(some, row_sum, 1.0))
                per = rows // 4
                for p in range(4):
                    o_out[4 * i + p, pl.ds(0, per), cols] = mixed[p * per : (p + 1) * per].astype(BF)
                lse = jnp.where(some, row_max + jnp.log2(jnp.where(some, row_sum, 1.0)), LOW)
                wide = jnp.broadcast_to(lse, (rows, rows))
                eye = lax.broadcasted_iota(jnp.int32, (rows, rows), 0) == lax.broadcasted_iota(
                    jnp.int32, (rows, rows), 1
                )
                lse_rows.append(jnp.sum(jnp.where(eye, wide, 0.0), axis=0, keepdims=True))
            else:
                acc_out[i, :, cols] = weighted
                stat_new = jnp.where(lane == j, row_max, stat_new)
                stat_new = jnp.where(lane == 2 + j, row_sum, stat_new)
        if last:
            tail = tail_block(lse_rows, rows)
            for p in range(4):
                o_out[4 * i + p, pl.ds(rows // 4, TAIL), :] = tail
        else:
            stat_out[i] = stat_new


def attend(info, q_all, kvs, state, own, last, name, tiles=2):
    count, padded, width = q_all.shape
    rows = padded - TAIL
    first = state is None
    grid = count // tiles
    blocks = len(kvs)
    tile_map = lambda g, info: (g, 0, 0)
    whole = lambda g, info: (0, 0, 0)
    in_specs = [
        pl.BlockSpec((tiles, padded, width), tile_map),
        pl.BlockSpec((1, TAIL, width), lambda g, info: (0, rows // TAIL, 0)),
    ]
    in_specs += [pl.BlockSpec((2, padded, width), whole)] * blocks
    operands = [q_all, q_all, *kvs]
    state_specs = [
        pl.BlockSpec((tiles, rows, width), tile_map),
        pl.BlockSpec((tiles, rows, HEAD_DIM), tile_map),
    ]
    aliases = {}
    if not first:
        in_specs += state_specs
        operands += list(state)
        if not last:
            aliases = {1 + len(operands) - 2: 0, 1 + len(operands) - 1: 1}
    if last:
        out_specs = pl.BlockSpec((4 * tiles, rows // 4 + TAIL, width), tile_map)
        out_shape = jax.ShapeDtypeStruct((4 * count, rows // 4 + TAIL, width), BF)
    else:
        out_specs = state_specs
        out_shape = [
            jax.ShapeDtypeStruct((count, rows, width), F32),
            jax.ShapeDtypeStruct((count, rows, HEAD_DIM), F32),
        ]
    scores = count * rows * 2 * blocks * 2 * rows
    return pl.pallas_call(
        functools.partial(
            attend_kernel, blocks=blocks, own=own, first=first, last=last, tiles=tiles, rows=rows
        ),
        grid_spec=pltpu.PrefetchScalarGridSpec(
            num_scalar_prefetch=1, grid=(grid,), in_specs=in_specs, out_specs=out_specs
        ),
        out_shape=out_shape,
        input_output_aliases=aliases,
        cost_estimate=pl.CostEstimate(
            flops=scores * 768, transcendentals=scores, bytes_accessed=6_000_000
        ),
        compiler_params=pltpu.CompilerParams(
            dimension_semantics=("arbitrary",), vmem_limit_bytes=40 * 1024 * 1024
        ),
        name=name,
    )(info, *operands)


def post_kernel(
    tp_ref, part_ref, w_ref, res_ref, gain_ref, ids_ref, stream_out, normed_out, send_out, att, strm
):
    step = pl.program_id(0)
    sources = part_ref.shape[0]
    own_rows = res_ref.shape[0]
    width = part_ref.shape[2]
    groups = att.shape[1] // width
    ys = sources // groups

    @pl.when(step == 0)
    def _():
        pick = lax.broadcasted_iota(jnp.int32, (own_rows, width), 1) == (
            tp_ref[0] * own_rows + lax.broadcasted_iota(jnp.int32, (own_rows, width), 0)
        )
        for g in range(groups):
            core, tp = g // (groups // 2), g % (groups // 2)
            col = (tp * 2 + core) * width
            tails = [part_ref[y * groups + g, own_rows:, :].astype(F32) for y in range(ys)]
            for j in range(2):
                sums = []
                for y in range(ys):
                    row = row_of(tails[y], j)
                    sums.append(jnp.sum(jnp.where(pick, row, 0.0), axis=1, keepdims=True))
                top = sums[0]
                for s in sums[1:]:
                    top = jnp.maximum(top, s)
                weights = [jnp.exp2(s - top) for s in sums]
                total = weights[0]
                for w in weights[1:]:
                    total = total + w
                inverse = 1.0 / total
                mixed = None
                for y in range(ys):
                    part = part_ref[
                        y * groups + g, pl.ds(0, own_rows), pl.ds(j * HEAD_DIM, HEAD_DIM)
                    ].astype(F32) * (weights[y] * inverse)
                    mixed = part if mixed is None else mixed + part
                att[:, pl.ds(col + j * HEAD_DIM, HEAD_DIM)] = mixed.astype(BF)

    block = w_ref.shape[1]
    cols = pl.ds(pl.multiple_of(step * block, block), block)
    branch = jnp.dot(att[...], w_ref[...], preferred_element_type=F32)
    stream = (res_ref[...].astype(F32) + branch).astype(BF)
    stream_out[...] = stream
    strm[:, cols] = stream

    @pl.when(step == pl.num_programs(0) - 1)
    def _():
        wide = strm[...].astype(F32)
        mean = jnp.mean(wide * wide, axis=1, keepdims=True)
        normed = (wide * lax.rsqrt(mean + NORM_EPS) * gain_ref[...]).astype(BF)
        normed_out[...] = normed
        experts = send_out.shape[0]
        cap = send_out.shape[1]
        expert = lax.broadcasted_iota(jnp.int32, (experts, own_rows), 0)
        named = jnp.zeros((experts, own_rows), F32)
        for k in range(TOPK):
            named = jnp.where(ids_ref[k : k + 1, :] == expert, 1.0, named)
        earlier = (
            lax.broadcasted_iota(jnp.int32, (own_rows, own_rows), 0)
            < lax.broadcasted_iota(jnp.int32, (own_rows, own_rows), 1)
        ).astype(BF)
        rank = jnp.dot(named.astype(BF), earlier, preferred_element_type=F32)
        rank = jnp.where(named > 0.5, rank, -1.0)
        slot = lax.broadcasted_iota(jnp.int32, (experts, cap, own_rows), 1).astype(F32)
        chosen = (rank[:, None, :] == slot).astype(F32).reshape(experts * cap, own_rows).astype(BF)
        sent = jnp.dot(chosen, normed, preferred_element_type=F32).astype(BF)
        send_out[...] = sent.reshape(send_out.shape)


def post(tp, parts, weight, residual, gain, ids_t, experts, cap):
    rows, width = residual.shape
    block = 256
    fixed2 = lambda g, tp: (0, 0)
    fixed3 = lambda g, tp: (0, 0, 0)
    tiled = lambda g, tp: (0, g)
    return pl.pallas_call(
        post_kernel,
        grid_spec=pltpu.PrefetchScalarGridSpec(
            num_scalar_prefetch=1,
            grid=(width // block,),
            in_specs=[
                pl.BlockSpec(parts.shape, fixed3),
                pl.BlockSpec((width, block), tiled),
                pl.BlockSpec((rows, block), tiled),
                pl.BlockSpec((1, width), fixed2),
                pl.BlockSpec(ids_t.shape, fixed2),
            ],
            out_specs=[
                pl.BlockSpec((rows, block), tiled),
                pl.BlockSpec((rows, width), fixed2),
                pl.BlockSpec((experts, cap, width), fixed3),
            ],
            scratch_shapes=[pltpu.VMEM((rows, width), BF), pltpu.VMEM((rows, width), BF)],
        ),
        out_shape=[
            jax.ShapeDtypeStruct((rows, width), BF),
            jax.ShapeDtypeStruct((rows, width), BF),
            jax.ShapeDtypeStruct((experts, cap, width), BF),
        ],
        compiler_params=pltpu.CompilerParams(
            dimension_semantics=("arbitrary",), vmem_limit_bytes=40 * 1024 * 1024
        ),
        name="post",
    )(tp, parts, weight, residual, gain, ids_t)


def finish_kernel(res_ref, base_ref, ids_ref, route_ref, out_ref):
    rows = base_ref.shape[0]
    experts, cap, width = res_ref.shape
    slots = experts * cap
    route = route_ref[...]
    gates = route / jnp.sum(route, axis=1, keepdims=True) * ROUTED_SCALE
    expert = lax.broadcasted_iota(jnp.int32, (rows, experts), 1)
    named = jnp.zeros((rows, experts), F32)
    gate = jnp.zeros((rows, experts), F32)
    for k in range(TOPK):
        here = ids_ref[:, k : k + 1] == expert
        named = jnp.where(here, 1.0, named)
        gate = jnp.where(here, gates[:, k : k + 1], gate)
    earlier = (
        lax.broadcasted_iota(jnp.int32, (rows, rows), 1)
        < lax.broadcasted_iota(jnp.int32, (rows, rows), 0)
    ).astype(BF)
    rank = jnp.dot(earlier, named.astype(BF), preferred_element_type=F32)
    rank = jnp.where(named > 0.5, rank, 128.0)
    slot = lax.broadcasted_iota(jnp.int32, (experts, slots), 1)
    first = lax.broadcasted_iota(jnp.int32, (experts, slots), 0) * cap
    spread = ((slot >= first) & (slot < first + cap)).astype(BF)
    rank_x = jnp.dot(rank.astype(BF), spread, preferred_element_type=F32)
    place = (lax.broadcasted_iota(jnp.int32, (rows, slots), 1) % cap).astype(F32)
    chosen = rank_x == place
    high = gate.astype(BF)
    low = (gate - high.astype(F32)).astype(BF)
    high_x = jnp.where(chosen, jnp.dot(high, spread, preferred_element_type=F32), 0.0).astype(BF)
    low_x = jnp.where(chosen, jnp.dot(low, spread, preferred_element_type=F32), 0.0).astype(BF)
    results = res_ref[...].reshape(slots, width)
    routed = jnp.dot(high_x, results, preferred_element_type=F32) + jnp.dot(
        low_x, results, preferred_element_type=F32
    )
    out_ref[...] = (base_ref[...] + routed).astype(BF)


def finish(results, base, ids, route):
    return pl.pallas_call(
        finish_kernel,
        out_shape=jax.ShapeDtypeStruct(base.shape, BF),
        compiler_params=pltpu.CompilerParams(vmem_limit_bytes=40 * 1024 * 1024),
        name="finish",
    )(results, base, ids, route)


def local(
    residual,
    queries,
    key_rows,
    value_rows,
    forget_sums,
    out_weight,
    norm_gain,
    expert_ids,
    route_weights,
    expert_gate,
    expert_up,
    expert_down,
    shared_gate,
    shared_up,
    shared_down,
):
    z_count = lax.axis_size("z")
    y_count = lax.axis_size("y")
    z = lax.axis_index("z")
    y = lax.axis_index("y")
    rows = queries.shape[0]
    experts = z_count * y_count * 2
    cap = 2 * residual.shape[0] * TOPK // experts

    weight = lax.all_gather(out_weight, "tp", axis=0, tiled=True)
    kv_send, q_send = pack(queries, key_rows, value_rows, forget_sums.T, y_count)
    own = lax.all_to_all(kv_send, "c", split_axis=0, concat_axis=0)
    up_ring = [(i, (i + 1) % z_count) for i in range(z_count)]
    down_ring = [(i, (i - 1) % z_count) for i in range(z_count)]
    half = z_count // 2
    ups, downs = [own], [own]
    for s in range(1, half + 1):
        ups.append(lax.ppermute(ups[-1], "z", up_ring))
        if s < half:
            downs.append(lax.ppermute(downs[-1], "z", down_ring))
    q_all = lax.all_to_all(q_send, ("y", "c"), split_axis=0, concat_axis=0)

    def flags(*steps):
        good = []
        for direction, s in steps:
            if s == 0:
                good.append(jnp.int32(1))
            elif direction > 0:
                good.append((z >= s).astype(jnp.int32))
            else:
                good.append((z + s >= z_count).astype(jnp.int32))
        return jnp.stack([2 * y * rows, *good]).astype(jnp.int32)

    state = attend(
        flags((1, 0), (1, 1), (-1, 1)), q_all, [own, ups[1], downs[1]], None, True, False, "attend1"
    )
    for s in range(2, half):
        state = attend(
            flags((1, s), (-1, s)), q_all, [ups[s], downs[s]], state, False, False, f"attend{s}"
        )
    sent = attend(flags((1, half)), q_all, [ups[half]], state, False, True, "attend_last")
    parts = lax.all_to_all(sent, ("y", "c", "tp"), split_axis=0, concat_axis=0)
    tp = lax.axis_index("tp").astype(jnp.int32).reshape(1)
    stream, normed, outgoing = post(
        tp, parts, weight, residual, norm_gain[None, :], expert_ids.T, experts, cap
    )
    arrived = lax.all_to_all(outgoing, ("z", "y", "c"), split_axis=0, concat_axis=0)
    shared_hidden = (
        jax.nn.silu(jnp.dot(normed, shared_gate, preferred_element_type=F32))
        * jnp.dot(normed, shared_up, preferred_element_type=F32)
    ).astype(BF)
    base = stream.astype(F32) + jnp.dot(shared_hidden, shared_down, preferred_element_type=F32)
    tokens = arrived.reshape(experts * cap, -1)
    gate_part = jnp.dot(tokens, expert_gate[0], preferred_element_type=F32)
    up_part = jnp.dot(tokens, expert_up[0], preferred_element_type=F32)
    hidden = (jax.nn.silu(gate_part) * up_part).astype(BF)
    processed = jnp.dot(hidden, expert_down[0], preferred_element_type=F32).astype(BF)
    returned = lax.all_to_all(
        processed.reshape(arrived.shape), ("z", "y", "c"), split_axis=0, concat_axis=0
    )
    return finish(returned, base, expert_ids, route_weights)


def solution(mesh):
    sp = mesh.shape["sp"]
    tp = mesh.shape["tp"]
    grid = Mesh(mesh.devices.reshape(8, sp // 16, 2, tp), ("z", "y", "c", "tp"))
    seq = ("z", "y", "c")
    in_specs = (
        P((*seq, "tp"), None),
        P(seq, "tp"),
        P(seq, "tp"),
        P(seq, "tp"),
        P(seq, "tp"),
        P("tp", None),
        P(),
        P((*seq, "tp"), None),
        P((*seq, "tp"), None),
        P(seq, None, None),
        P(seq, None, None),
        P(seq, None, None),
        P(),
        P(),
        P(),
    )
    out_specs = P((*seq, "tp"), None)
    return jax.shard_map(local, mesh=grid, in_specs=in_specs, out_specs=out_specs, check_vma=False)
```

```python
import functools
import math

import jax
import jax.numpy as jnp
from jax import lax
from jax.experimental import pallas as pl
from jax.experimental.pallas import tpu as pltpu
from jax.sharding import Mesh, PartitionSpec as P

HEADS = 16
KV_HEADS = 8
HEAD_DIM = 128
TOPK = 4
ROUTED_SCALE = 2.5
NORM_EPS = 1e-06
LOG2E = math.log2(math.e)
SCORE2 = HEAD_DIM**-0.5 * LOG2E
LOW = -1e30
TAIL = 8

BF = jnp.bfloat16
F32 = jnp.float32


def pieces(row):
    high = row.astype(BF)
    rest = row - high.astype(F32)
    mid = rest.astype(BF)
    low = (rest - mid.astype(F32)).astype(BF)
    return [high.astype(F32), mid.astype(F32), low.astype(F32)]


def tail_block(rows, width):
    parts = [piece for row in rows for piece in pieces(row)]
    parts.append(jnp.zeros((TAIL - len(parts), width), F32))
    return jnp.concatenate(parts, axis=0).astype(BF)


def row_of(tail, j):
    return tail[3 * j : 3 * j + 1] + tail[3 * j + 1 : 3 * j + 2] + tail[3 * j + 2 : 3 * j + 3]


def pack_kernel(q_ref, k_ref, v_ref, f_ref, kv_out, q_out):
    rows = q_ref.shape[0]
    ys = q_out.shape[0] // 2
    for c in range(2):
        tail = tail_block([f_ref[2 * c : 2 * c + 1, :], f_ref[2 * c + 1 : 2 * c + 2, :]], rows)
        kv_out[c, :rows, :HEAD_DIM] = k_ref[:, c * HEAD_DIM : (c + 1) * HEAD_DIM]
        kv_out[c, :rows, HEAD_DIM:] = v_ref[:, c * HEAD_DIM : (c + 1) * HEAD_DIM]
        kv_out[c, rows:, :] = tail
        q_part = q_ref[:, c * 2 * HEAD_DIM : (c + 1) * 2 * HEAD_DIM]
        for y in range(ys):
            q_out[2 * y + c, :rows, :] = q_part
            q_out[2 * y + c, rows:, :] = tail


def pack(q, k, v, f_t, ys):
    rows = q.shape[0]
    width = 2 * HEAD_DIM
    return pl.pallas_call(
        pack_kernel,
        out_shape=(
            jax.ShapeDtypeStruct((2, rows + TAIL, width), BF),
            jax.ShapeDtypeStruct((2 * ys, rows + TAIL, width), BF),
        ),
        name="pack",
    )(q, k, v, f_t)


def attend_kernel(info, *refs, blocks, own, first, last, tiles, rows):
    q_ref, ref_tail = refs[0], refs[1]
    kv_refs = refs[2 : 2 + blocks]
    at = 2 + blocks
    if not first:
        acc_in, stat_in = refs[at], refs[at + 1]
        at += 2
    if last:
        (o_out,) = refs[at : at + 1]
    else:
        acc_out, stat_out = refs[at : at + 2]
    step = pl.program_id(0)
    first_tail = ref_tail[0].astype(F32)
    keys, values, biases = [], [], []
    ones = jnp.ones((rows, HEAD_DIM), BF)
    for b in range(blocks):
        for c in range(2):
            keys.append(kv_refs[b].at[c, pl.ds(0, rows), pl.ds(0, HEAD_DIM)])
            values.append(kv_refs[b].at[c, pl.ds(0, rows), pl.ds(HEAD_DIM, HEAD_DIM)])
            tail = kv_refs[b][c, rows:, :].astype(F32)
            pair = []
            for j in range(2):
                bias = (row_of(first_tail, j)[:, :1] - row_of(tail, j)) * LOG2E
                pair.append(jnp.where(info[1 + b] > 0, bias, -jnp.inf))
            biases.append(pair)
    lane = lax.broadcasted_iota(jnp.int32, (rows, HEAD_DIM), 1)

    def score_tiles(i):
        both = jnp.concatenate(
            [q_ref[i, pl.ds(0, rows), pl.ds(j * HEAD_DIM, HEAD_DIM)] for j in range(2)], axis=0
        )
        found = [[], []]
        for u in range(2 * blocks):
            raw = lax.dot_general(
                both, keys[u][...], (((1,), (1,)), ((), ())), preferred_element_type=F32
            )
            for j in range(2):
                score = raw[j * rows : (j + 1) * rows] * SCORE2 + biases[u][j]
                if own and u < 2:
                    q_pos = (step * tiles + i) * rows + lax.broadcasted_iota(
                        jnp.int32, (rows, rows), 0
                    )
                    k_pos = info[0] + u * rows + lax.broadcasted_iota(jnp.int32, (rows, rows), 1)
                    score = jnp.where(q_pos >= k_pos, score, -jnp.inf)
                found[j].append(score)
        return found

    def absorb(i, scores):
        maxes, olds = [], []
        for j in range(2):
            top = scores[j][0]
            for score in scores[j][1:]:
                top = jnp.maximum(top, score)
            row_max = jnp.max(top, axis=1, keepdims=True)
            old_max = LOW if first else stat_in[i, :, j : j + 1]
            olds.append(old_max)
            maxes.append(jnp.maximum(row_max, old_max))
        total = None
        for u in range(2 * blocks):
            weights = jnp.concatenate(
                [jnp.exp2(scores[j][u] - maxes[j]).astype(BF) for j in range(2)], axis=0
            )
            value = jnp.concatenate([values[u][...], ones], axis=1)
            part = jnp.dot(weights, value, preferred_element_type=F32)
            total = part if total is None else total + part
        stat_new = jnp.zeros((rows, HEAD_DIM), F32)
        lse_rows = []
        for j in range(2):
            cols = pl.ds(j * HEAD_DIM, HEAD_DIM)
            weighted = total[j * rows : (j + 1) * rows, :HEAD_DIM]
            row_sum = total[j * rows : (j + 1) * rows, HEAD_DIM:]
            if not first:
                factor = jnp.exp2(olds[j] - maxes[j])
                weighted = weighted + acc_in[i, :, cols] * factor
                row_sum = row_sum + stat_in[i, :, 2 + j : 3 + j] * factor
            if last:
                some = row_sum > 0.0
                row_sum = jnp.where(some, row_sum, 1.0)
                mixed = weighted * (1.0 / row_sum)
                per = rows // 4
                for p in range(4):
                    o_out[4 * i + p, pl.ds(0, per), cols] = mixed[p * per : (p + 1) * per].astype(BF)
                lse = jnp.where(some, maxes[j] + jnp.log2(row_sum), LOW)
                flat = []
                eye = lax.broadcasted_iota(jnp.int32, (HEAD_DIM, HEAD_DIM), 0) == (
                    lax.broadcasted_iota(jnp.int32, (HEAD_DIM, HEAD_DIM), 1)
                )
                for at in range(0, rows, HEAD_DIM):
                    flat.append(
                        jnp.sum(jnp.where(eye, lse[at : at + HEAD_DIM], 0.0), axis=0, keepdims=True)
                    )
                lse_rows.append(jnp.concatenate(flat, axis=1))
            else:
                acc_out[i, :, cols] = weighted
                stat_new = jnp.where(lane == j, maxes[j], stat_new)
                stat_new = jnp.where(lane == 2 + j, row_sum, stat_new)
        if last:
            tail = tail_block(lse_rows, rows)
            for p in range(4):
                o_out[4 * i + p, pl.ds(rows // 4, TAIL), :] = tail
        else:
            stat_out[i] = stat_new

    pending = score_tiles(0)
    for i in range(tiles):
        following = score_tiles(i + 1) if i + 1 < tiles else None
        absorb(i, pending)
        pending = following


def attend(info, q_all, kvs, state, own, last, name, tiles=4):
    count, padded, width = q_all.shape
    rows = padded - TAIL
    first = state is None
    grid = count // tiles
    blocks = len(kvs)
    tile_map = lambda g, info: (g, 0, 0)
    whole = lambda g, info: (0, 0, 0)
    in_specs = [
        pl.BlockSpec((tiles, padded, width), tile_map),
        pl.BlockSpec((1, TAIL, width), lambda g, info: (0, rows // TAIL, 0)),
    ]
    in_specs += [pl.BlockSpec((2, padded, width), whole)] * blocks
    operands = [q_all, q_all, *kvs]
    state_specs = [
        pl.BlockSpec((tiles, rows, width), tile_map),
        pl.BlockSpec((tiles, rows, HEAD_DIM), tile_map),
    ]
    aliases = {}
    if not first:
        in_specs += state_specs
        operands += list(state)
        if not last:
            aliases = {1 + len(operands) - 2: 0, 1 + len(operands) - 1: 1}
    if last:
        out_specs = pl.BlockSpec((4 * tiles, rows // 4 + TAIL, width), tile_map)
        out_shape = jax.ShapeDtypeStruct((4 * count, rows // 4 + TAIL, width), BF)
    else:
        out_specs = state_specs
        out_shape = [
            jax.ShapeDtypeStruct((count, rows, width), F32),
            jax.ShapeDtypeStruct((count, rows, HEAD_DIM), F32),
        ]
    scores = count * rows * 2 * blocks * 2 * rows
    return pl.pallas_call(
        functools.partial(
            attend_kernel, blocks=blocks, own=own, first=first, last=last, tiles=tiles, rows=rows
        ),
        grid_spec=pltpu.PrefetchScalarGridSpec(
            num_scalar_prefetch=1, grid=(grid,), in_specs=in_specs, out_specs=out_specs
        ),
        out_shape=out_shape,
        input_output_aliases=aliases,
        cost_estimate=pl.CostEstimate(
            flops=scores * 768, transcendentals=scores, bytes_accessed=6_000_000
        ),
        compiler_params=pltpu.CompilerParams(
            dimension_semantics=("arbitrary",), vmem_limit_bytes=40 * 1024 * 1024
        ),
        name=name,
    )(info, *operands)


def post_kernel(
    place,
    part_ref,
    w_own_ref,
    w_other_ref,
    res_ref,
    gain_ref,
    ids_ref,
    stream_out,
    normed_out,
    send_out,
    att,
    strm,
):
    step = pl.program_id(0)
    sources = part_ref.shape[0]
    own_rows = res_ref.shape[0]
    width = part_ref.shape[2]
    groups = att.shape[1] // width
    ys = sources // groups

    @pl.when(step == 0)
    def _():
        pick = lax.broadcasted_iota(jnp.int32, (own_rows, width), 1) == (
            place[0] * own_rows + lax.broadcasted_iota(jnp.int32, (own_rows, width), 0)
        )
        for g in range(groups):
            source = ((g // (groups // 2)) ^ place[1]) * (groups // 2) + g % (groups // 2)
            col = g * width
            tails = [part_ref[y * groups + source, own_rows:, :].astype(F32) for y in range(ys)]
            for j in range(2):
                sums = []
                for y in range(ys):
                    row = row_of(tails[y], j)
                    sums.append(jnp.sum(jnp.where(pick, row, 0.0), axis=1, keepdims=True))
                top = sums[0]
                for s in sums[1:]:
                    top = jnp.maximum(top, s)
                weights = [jnp.exp2(s - top) for s in sums]
                total = weights[0]
                for w in weights[1:]:
                    total = total + w
                inverse = 1.0 / total
                mixed = None
                for y in range(ys):
                    part = part_ref[
                        y * groups + source, pl.ds(0, own_rows), pl.ds(j * HEAD_DIM, HEAD_DIM)
                    ].astype(F32) * (weights[y] * inverse)
                    mixed = part if mixed is None else mixed + part
                att[:, pl.ds(col + j * HEAD_DIM, HEAD_DIM)] = mixed.astype(BF)

    block = w_own_ref.shape[1]
    half = w_own_ref.shape[0]
    cols = pl.ds(pl.multiple_of(step * block, block), block)
    branch = jnp.dot(att[:, :half], w_own_ref[...], preferred_element_type=F32) + jnp.dot(
        att[:, half:], w_other_ref[...], preferred_element_type=F32
    )
    stream = (res_ref[...].astype(F32) + branch).astype(BF)
    stream_out[...] = stream
    strm[:, cols] = stream

    @pl.when(step == pl.num_programs(0) - 1)
    def _():
        wide = strm[...].astype(F32)
        mean = jnp.mean(wide * wide, axis=1, keepdims=True)
        normed = (wide * lax.rsqrt(mean + NORM_EPS) * gain_ref[...]).astype(BF)
        normed_out[...] = normed
        experts = send_out.shape[0]
        cap = send_out.shape[1]
        expert = lax.broadcasted_iota(jnp.int32, (experts, own_rows), 0)
        named = jnp.zeros((experts, own_rows), F32)
        for k in range(TOPK):
            named = jnp.where(ids_ref[k : k + 1, :] == expert, 1.0, named)
        earlier = (
            lax.broadcasted_iota(jnp.int32, (own_rows, own_rows), 0)
            < lax.broadcasted_iota(jnp.int32, (own_rows, own_rows), 1)
        ).astype(BF)
        rank = jnp.dot(named.astype(BF), earlier, preferred_element_type=F32)
        rank = jnp.where(named > 0.5, rank, -1.0)
        slot = lax.broadcasted_iota(jnp.int32, (experts, cap, own_rows), 1).astype(F32)
        chosen = (rank[:, None, :] == slot).astype(F32).reshape(experts * cap, own_rows).astype(BF)
        sent = jnp.dot(chosen, normed, preferred_element_type=F32).astype(BF)
        send_out[...] = sent.reshape(send_out.shape)


def post(place, parts, w_own, w_other, residual, gain, ids_t, experts, cap):
    rows, width = residual.shape
    block = 256
    fixed2 = lambda g, place: (0, 0)
    fixed3 = lambda g, place: (0, 0, 0)
    tiled = lambda g, place: (0, g)
    return pl.pallas_call(
        post_kernel,
        grid_spec=pltpu.PrefetchScalarGridSpec(
            num_scalar_prefetch=1,
            grid=(width // block,),
            in_specs=[
                pl.BlockSpec(parts.shape, fixed3),
                pl.BlockSpec((width // 2, block), tiled),
                pl.BlockSpec((width // 2, block), tiled),
                pl.BlockSpec((rows, block), tiled),
                pl.BlockSpec((1, width), fixed2),
                pl.BlockSpec(ids_t.shape, fixed2),
            ],
            out_specs=[
                pl.BlockSpec((rows, block), tiled),
                pl.BlockSpec((rows, width), fixed2),
                pl.BlockSpec((experts, cap, width), fixed3),
            ],
            scratch_shapes=[pltpu.VMEM((rows, width), BF), pltpu.VMEM((rows, width), BF)],
        ),
        out_shape=[
            jax.ShapeDtypeStruct((rows, width), BF),
            jax.ShapeDtypeStruct((rows, width), BF),
            jax.ShapeDtypeStruct((experts, cap, width), BF),
        ],
        compiler_params=pltpu.CompilerParams(
            dimension_semantics=("arbitrary",), vmem_limit_bytes=40 * 1024 * 1024
        ),
        name="post",
    )(place, parts, w_own, w_other, residual, gain, ids_t)


def expert_kernel(x_ref, gate_ref, up_ref, down_ref, out_ref):
    peers, cap, width = x_ref.shape
    x = x_ref[...].reshape(peers * cap, width)
    gate = jnp.dot(x, gate_ref[0], preferred_element_type=F32)
    up = jnp.dot(x, up_ref[0], preferred_element_type=F32)
    hidden = (gate / (1.0 + jnp.exp(-gate)) * up).astype(BF)
    out = jnp.dot(hidden, down_ref[0], preferred_element_type=F32).astype(BF)
    out_ref[...] = out.reshape(peers, cap, width)


def expert(arrived, gate, up, down, steps=4):
    peers, cap, width = arrived.shape
    rows = pl.BlockSpec((peers // steps, cap, width), lambda g: (g, 0, 0))
    whole = lambda g: (0, 0, 0)
    return pl.pallas_call(
        expert_kernel,
        grid=(steps,),
        in_specs=[
            rows,
            pl.BlockSpec(gate.shape, whole),
            pl.BlockSpec(up.shape, whole),
            pl.BlockSpec(down.shape, whole),
        ],
        out_specs=rows,
        out_shape=jax.ShapeDtypeStruct(arrived.shape, BF),
        compiler_params=pltpu.CompilerParams(
            dimension_semantics=("arbitrary",), vmem_limit_bytes=40 * 1024 * 1024
        ),
        name="expert",
    )(arrived, gate, up, down)


def finish_kernel(res_ref, base_ref, ids_ref, route_ref, out_ref):
    rows = base_ref.shape[0]
    experts, cap, width = res_ref.shape
    slots = experts * cap
    route = route_ref[...]
    gates = route / jnp.sum(route, axis=1, keepdims=True) * ROUTED_SCALE
    expert = lax.broadcasted_iota(jnp.int32, (rows, experts), 1)
    named = jnp.zeros((rows, experts), F32)
    gate = jnp.zeros((rows, experts), F32)
    for k in range(TOPK):
        here = ids_ref[:, k : k + 1] == expert
        named = jnp.where(here, 1.0, named)
        gate = jnp.where(here, gates[:, k : k + 1], gate)
    earlier = (
        lax.broadcasted_iota(jnp.int32, (rows, rows), 1)
        < lax.broadcasted_iota(jnp.int32, (rows, rows), 0)
    ).astype(BF)
    rank = jnp.dot(earlier, named.astype(BF), preferred_element_type=F32)
    rank = jnp.where(named > 0.5, rank, 128.0)
    slot = lax.broadcasted_iota(jnp.int32, (experts, slots), 1)
    first = lax.broadcasted_iota(jnp.int32, (experts, slots), 0) * cap
    spread = ((slot >= first) & (slot < first + cap)).astype(BF)
    rank_x = jnp.dot(rank.astype(BF), spread, preferred_element_type=F32)
    place = (lax.broadcasted_iota(jnp.int32, (rows, slots), 1) % cap).astype(F32)
    chosen = rank_x == place
    high = gate.astype(BF)
    low = (gate - high.astype(F32)).astype(BF)
    high_x = jnp.where(chosen, jnp.dot(high, spread, preferred_element_type=F32), 0.0).astype(BF)
    low_x = jnp.where(chosen, jnp.dot(low, spread, preferred_element_type=F32), 0.0).astype(BF)
    results = res_ref[...].reshape(slots, width)
    routed = jnp.dot(high_x, results, preferred_element_type=F32) + jnp.dot(
        low_x, results, preferred_element_type=F32
    )
    out_ref[...] = (base_ref[...] + routed).astype(BF)


def finish(results, base, ids, route):
    return pl.pallas_call(
        finish_kernel,
        out_shape=jax.ShapeDtypeStruct(base.shape, BF),
        compiler_params=pltpu.CompilerParams(vmem_limit_bytes=40 * 1024 * 1024),
        name="finish",
    )(results, base, ids, route)


def local(
    residual,
    queries,
    key_rows,
    value_rows,
    forget_sums,
    out_weight,
    norm_gain,
    expert_ids,
    route_weights,
    expert_gate,
    expert_up,
    expert_down,
    shared_gate,
    shared_up,
    shared_down,
):
    z_count = lax.axis_size("z")
    y_count = lax.axis_size("y")
    z = lax.axis_index("z")
    y = lax.axis_index("y")
    rows = queries.shape[0]
    experts = z_count * y_count * 2
    cap = 2 * residual.shape[0] * TOPK // experts

    core = lax.axis_index("c")
    half_rows = out_weight.shape[0] // 2
    own_part = lax.dynamic_slice_in_dim(out_weight, core * half_rows, half_rows, 0)
    w_own = lax.all_gather(own_part, "tp", axis=0, tiled=True)
    kv_send, q_send = pack(queries, key_rows, value_rows, forget_sums.T, y_count)
    own = lax.all_to_all(kv_send, "c", split_axis=0, concat_axis=0)
    up_ring = [(i, (i + 1) % z_count) for i in range(z_count)]
    down_ring = [(i, (i - 1) % z_count) for i in range(z_count)]
    q_all = lax.all_to_all(q_send, ("y", "c"), split_axis=0, concat_axis=0)

    def up(block):
        return lax.ppermute(block, "z", up_ring)

    def down(block):
        return lax.ppermute(block, "z", down_ring)

    def flags(*steps):
        good = [(z >= s) if s >= 0 else (z - s >= z_count) for s in steps]
        return jnp.stack([2 * y * rows, *good]).astype(jnp.int32)

    up1, down1 = up(own), down(own)
    up2, down2 = up(up1), down(down1)
    up3, down3 = up(up2), down(down2)
    state = attend(flags(0, 1, -1), q_all, [own, up1, down1], None, True, False, "attend1")
    state, up3, down3 = lax.optimization_barrier((state, up3, down3))
    up4 = up(up3)
    state = attend(flags(2, -2), q_all, [up2, down2], state, False, False, "attend2")
    sent = attend(flags(3, -3, 4), q_all, [up3, down3, up4], state, False, True, "attend3")
    sent, w_own = lax.optimization_barrier((sent, w_own))
    w_other = lax.ppermute(w_own, "c", [(0, 1), (1, 0)])
    parts = lax.all_to_all(sent, ("y", "c", "tp"), split_axis=0, concat_axis=0)
    place = jnp.stack([lax.axis_index("tp"), core]).astype(jnp.int32)
    stream, normed, outgoing = post(
        place, parts, w_own, w_other, residual, norm_gain[None, :], expert_ids.T, experts, cap
    )
    arrived = lax.all_to_all(outgoing, ("z", "y", "c"), split_axis=0, concat_axis=0)
    shared_hidden = (
        jax.nn.silu(jnp.dot(normed, shared_gate, preferred_element_type=F32))
        * jnp.dot(normed, shared_up, preferred_element_type=F32)
    ).astype(BF)
    base = stream.astype(F32) + jnp.dot(shared_hidden, shared_down, preferred_element_type=F32)
    processed = expert(arrived, expert_gate, expert_up, expert_down)
    returned = lax.all_to_all(
        processed, ("z", "y", "c"), split_axis=0, concat_axis=0
    )
    return finish(returned, base, expert_ids, route_weights)


def solution(mesh):
    sp = mesh.shape["sp"]
    tp = mesh.shape["tp"]
    grid = Mesh(mesh.devices.reshape(8, sp // 16, 2, tp), ("z", "y", "c", "tp"))
    seq = ("z", "y", "c")
    in_specs = (
        P((*seq, "tp"), None),
        P(seq, "tp"),
        P(seq, "tp"),
        P(seq, "tp"),
        P(seq, "tp"),
        P("tp", None),
        P(),
        P((*seq, "tp"), None),
        P((*seq, "tp"), None),
        P(seq, None, None),
        P(seq, None, None),
        P(seq, None, None),
        P(),
        P(),
        P(),
    )
    out_specs = P((*seq, "tp"), None)
    return jax.shard_map(local, mesh=grid, in_specs=in_specs, out_specs=out_specs, check_vma=False)
```

```python
import functools
import math

import jax
import jax.numpy as jnp
from jax import lax
from jax.experimental import pallas as pl
from jax.experimental.pallas import tpu as pltpu
from jax.sharding import Mesh, PartitionSpec as P

HEAD_DIM = 128
TOPK = 4
ROUTED_SCALE = 2.5
NORM_EPS = 1e-06
LOG2E = math.log2(math.e)
SCORE2 = HEAD_DIM**-0.5 * LOG2E
LOW = -1e30
TAIL = 8

BF = jnp.bfloat16
F32 = jnp.float32


def pieces(row):
    high = row.astype(BF)
    rest = row - high.astype(F32)
    mid = rest.astype(BF)
    low = (rest - mid.astype(F32)).astype(BF)
    return [high.astype(F32), mid.astype(F32), low.astype(F32)]


def tail_block(rows, width):
    parts = [piece for row in rows for piece in pieces(row)]
    parts.append(jnp.zeros((TAIL - len(parts), width), F32))
    return jnp.concatenate(parts, axis=0).astype(BF)


def row_of(tail, j):
    return tail[3 * j : 3 * j + 1] + tail[3 * j + 1 : 3 * j + 2] + tail[3 * j + 2 : 3 * j + 3]


def pack_keys_kernel(k_ref, v_ref, f_ref, out):
    rows = k_ref.shape[0]
    for c in range(2):
        out[c, :rows, :HEAD_DIM] = k_ref[:, c * HEAD_DIM : (c + 1) * HEAD_DIM]
        out[c, :rows, HEAD_DIM:] = v_ref[:, c * HEAD_DIM : (c + 1) * HEAD_DIM]
        out[c, rows:, :] = tail_block([f_ref[2 * c : 2 * c + 1, :], f_ref[2 * c + 1 : 2 * c + 2, :]], rows)


def pack_queries_kernel(q_ref, f_ref, _, out):
    rows = q_ref.shape[0]
    for c in range(2):
        tail = tail_block([f_ref[2 * c : 2 * c + 1, :], f_ref[2 * c + 1 : 2 * c + 2, :]], rows)
        part = q_ref[:, c * 2 * HEAD_DIM : (c + 1) * 2 * HEAD_DIM]
        for y in range(out.shape[0] // 2):
            out[2 * y + c, :rows, :] = part
            out[2 * y + c, rows:, :] = tail


def pack_keys(k, v, f_t):
    return pl.pallas_call(
        pack_keys_kernel,
        out_shape=pltpu.HBM((2, k.shape[0] + TAIL, 2 * HEAD_DIM), BF),
        name="pack_keys",
    )(k, v, f_t)


def pack_queries(q, f_t, after, ys):
    return pl.pallas_call(
        pack_queries_kernel,
        in_specs=[pl.BlockSpec(), pl.BlockSpec(), pl.BlockSpec(memory_space=pl.ANY)],
        out_shape=pltpu.HBM((2 * ys, q.shape[0] + TAIL, 2 * HEAD_DIM), BF),
        name="pack_queries",
    )(q, f_t, after)


def attend_kernel(info, *refs, steps, z_count, first, last, tiles, rows):
    blocks, own = len(steps), 0 in steps
    q_ref = refs[0]
    kv_refs = refs[1 : 1 + blocks]
    at = 1 + blocks
    if not first:
        acc_in, stat_in = refs[at], refs[at + 1]
        at += 2
    if last:
        (o_out,) = refs[at : at + 1]
    else:
        acc_out, stat_out = refs[at : at + 2]
    first_tail = q_ref[0, rows:, :].astype(F32)
    keys, values, biases = [], [], []
    ones = jnp.ones((rows, HEAD_DIM), BF)
    for b, s in enumerate(steps):
        valid = info[1] >= s if s >= 0 else info[1] - s >= z_count
        for c in range(2):
            keys.append(kv_refs[b].at[c, pl.ds(0, rows), pl.ds(0, HEAD_DIM)])
            values.append(kv_refs[b].at[c, pl.ds(0, rows), pl.ds(HEAD_DIM, HEAD_DIM)])
            tail = kv_refs[b][c, rows:, :].astype(F32)
            pair = []
            for j in range(2):
                bias = (row_of(first_tail, j)[:, :1] - row_of(tail, j)) * LOG2E
                pair.append(jnp.where(valid, bias, -jnp.inf))
            biases.append(pair)

    def score_tiles(i):
        both = jnp.concatenate(
            [q_ref[i, pl.ds(0, rows), pl.ds(j * HEAD_DIM, HEAD_DIM)] for j in range(2)], axis=0
        )
        found = [[], []]
        for u in range(2 * blocks):
            raw = lax.dot_general(
                both, keys[u][...], (((1,), (1,)), ((), ())), preferred_element_type=F32
            )
            for j in range(2):
                score = raw[j * rows : (j + 1) * rows] * SCORE2 + biases[u][j]
                if own and u < 2:
                    q_pos = i * rows + lax.broadcasted_iota(
                        jnp.int32, (rows, rows), 0
                    )
                    k_pos = info[0] + u * rows + lax.broadcasted_iota(jnp.int32, (rows, rows), 1)
                    score = jnp.where(q_pos >= k_pos, score, -jnp.inf)
                found[j].append(score)
        return found

    def absorb(i, scores):
        maxes, olds = [], []
        for j in range(2):
            top = scores[j][0]
            for score in scores[j][1:]:
                top = jnp.maximum(top, score)
            row_max = jnp.max(top, axis=1, keepdims=True)
            cols = pl.ds(j * HEAD_DIM, HEAD_DIM)
            old_max = jnp.full((rows, HEAD_DIM), LOW, F32) if first else stat_in[i, :, cols]
            olds.append(old_max)
            maxes.append(jnp.maximum(row_max, old_max))
        total = None
        wide = rows // HEAD_DIM
        for u in range(2 * blocks):
            weights = jnp.concatenate(
                [
                    jnp.exp2(scores[j][u] - jnp.concatenate([maxes[j]] * wide, axis=1)).astype(BF)
                    for j in range(2)
                ],
                axis=0,
            )
            value = jnp.concatenate([values[u][...], ones], axis=1)
            part = jnp.dot(weights, value, preferred_element_type=F32)
            total = part if total is None else total + part
        lse_rows = []
        for j in range(2):
            cols = pl.ds(j * HEAD_DIM, HEAD_DIM)
            weighted = total[j * rows : (j + 1) * rows, :HEAD_DIM]
            row_sum = total[j * rows : (j + 1) * rows, HEAD_DIM:]
            if not first:
                factor = jnp.exp2(olds[j] - maxes[j])
                sums = pl.ds((2 + j) * HEAD_DIM, HEAD_DIM)
                weighted = weighted + acc_in[i, :, cols] * factor
                row_sum = row_sum + acc_in[i, :, sums] * factor
            if last:
                some = row_sum > 0.0
                row_sum = jnp.where(some, row_sum, 1.0)
                mixed = weighted * (1.0 / row_sum)
                per = rows // 4
                for p in range(4):
                    o_out[4 * i + p, pl.ds(0, per), cols] = mixed[p * per : (p + 1) * per].astype(BF)
                lse = jnp.where(some, maxes[j] + jnp.log2(row_sum), LOW)
                flat = []
                eye = lax.broadcasted_iota(jnp.int32, (HEAD_DIM, HEAD_DIM), 0) == (
                    lax.broadcasted_iota(jnp.int32, (HEAD_DIM, HEAD_DIM), 1)
                )
                for at in range(0, rows, HEAD_DIM):
                    flat.append(
                        jnp.sum(jnp.where(eye, lse[at : at + HEAD_DIM], 0.0), axis=0, keepdims=True)
                    )
                lse_rows.append(jnp.concatenate(flat, axis=1))
            else:
                acc_out[i, :, cols] = weighted
                acc_out[i, :, pl.ds((2 + j) * HEAD_DIM, HEAD_DIM)] = row_sum
                stat_out[i, :, cols] = maxes[j]
        if last:
            tail = tail_block(lse_rows, rows)
            for p in range(4):
                o_out[4 * i + p, pl.ds(rows // 4, TAIL), :] = tail

    def some_tiles(step, _):
        pending = score_tiles(step * tiles)
        for n in range(tiles):
            i = step * tiles + n
            following = score_tiles(i + 1) if n + 1 < tiles else None
            absorb(i, pending)
            pending = following
        return 0

    lax.fori_loop(0, q_ref.shape[0] // tiles, some_tiles, 0)


def attend(info, q_all, kvs, steps, z_count, state, last, tiles=4):
    count, padded, width = q_all.shape
    rows = padded - TAIL
    first = state is None
    blocks = len(kvs)
    vmem = pl.BlockSpec(memory_space=pltpu.VMEM)
    operands = [q_all, *kvs]
    aliases = {}
    if not first:
        operands += list(state)
        if not last:
            aliases = {len(operands) - 1: 0, len(operands): 1}
    if last:
        out_shape = jax.ShapeDtypeStruct((4 * count, rows // 4 + TAIL, width), BF)
    else:
        out_shape = [
            jax.ShapeDtypeStruct((count, rows, 2 * width), F32),
            jax.ShapeDtypeStruct((count, rows, width), F32),
        ]
    scores = count * rows * 2 * blocks * 2 * rows
    return pl.pallas_call(
        functools.partial(
            attend_kernel, steps=steps, z_count=z_count, first=first, last=last, tiles=tiles, rows=rows
        ),
        in_specs=[pl.BlockSpec(memory_space=pltpu.SMEM)] + [vmem] * len(operands),
        out_specs=vmem if last else [vmem, vmem],
        out_shape=out_shape,
        input_output_aliases=aliases,
        cost_estimate=pl.CostEstimate(
            flops=scores * 768, transcendentals=scores, bytes_accessed=6_000_000
        ),
        compiler_params=pltpu.CompilerParams(vmem_limit_bytes=24 * 1024 * 1024),
    )(info, *operands)


def post_kernel(info, part_ref, *refs, turns, count):
    w_refs = refs[:count]
    res_ref, gain_ref, ids_ref, stream_out, normed_out, send_out, att, weight, sems = refs[count:]
    sources = part_ref.shape[0]
    own_rows = res_ref.shape[0]
    width = part_ref.shape[2]
    tps = len(turns)
    groups = 2 * tps
    ys = sources // groups
    copies = []
    at = 0
    for n, w_ref in enumerate(w_refs):
        size = w_ref.shape[0]
        copies.append(pltpu.make_async_copy(w_ref, weight.at[pl.ds(at, size)], sems.at[n]))
        copies[-1].start()
        at += size

    pick = lax.broadcasted_iota(jnp.int32, (own_rows, width), 1) == (
        info[2] * own_rows + lax.broadcasted_iota(jnp.int32, (own_rows, width), 0)
    )
    for s, turn in enumerate(turns):
        tp = (info[2] + turn) % tps
        for k in range(2):
            core = k if turn == 0 else info[3] ^ k
            col = (2 * s + k) * width
            index = core * tps + tp
            tails = [part_ref[y * groups + index, own_rows:, :].astype(F32) for y in range(ys)]
            for j in range(2):
                sums = []
                for y in range(ys):
                    row = row_of(tails[y], j)
                    sums.append(jnp.sum(jnp.where(pick, row, 0.0), axis=1, keepdims=True))
                top = sums[0]
                for one in sums[1:]:
                    top = jnp.maximum(top, one)
                weights = [jnp.exp2(one - top) for one in sums]
                total = weights[0]
                for w in weights[1:]:
                    total = total + w
                inverse = 1.0 / total
                mixed = None
                for y in range(ys):
                    part = part_ref[
                        y * groups + index, pl.ds(0, own_rows), pl.ds(j * HEAD_DIM, HEAD_DIM)
                    ].astype(F32) * (weights[y] * inverse)
                    mixed = part if mixed is None else mixed + part
                att[:, pl.ds(col + j * HEAD_DIM, HEAD_DIM)] = mixed.astype(BF)

    experts = send_out.shape[0]
    cap = send_out.shape[1]
    expert = lax.broadcasted_iota(jnp.int32, (experts, own_rows), 0)
    named = jnp.zeros((experts, own_rows), F32)
    for k in range(TOPK):
        named = jnp.where(ids_ref[k : k + 1, :] == expert, 1.0, named)
    earlier = (
        lax.broadcasted_iota(jnp.int32, (own_rows, own_rows), 0)
        < lax.broadcasted_iota(jnp.int32, (own_rows, own_rows), 1)
    ).astype(BF)
    rank = jnp.dot(named.astype(BF), earlier, preferred_element_type=F32)
    rank = jnp.where(named > 0.5, rank, -1.0)
    slot = lax.broadcasted_iota(jnp.int32, (experts, cap, own_rows), 1).astype(F32)
    chosen = (rank[:, None, :] == slot).astype(F32).reshape(experts * cap, own_rows).astype(BF)

    for copy in copies:
        copy.wait()
    block = 256
    squares = jnp.zeros((own_rows, 1), F32)
    for n in range(0, weight.shape[1], block):
        branch = jnp.dot(att[...], weight[:, n : n + block], preferred_element_type=F32)
        stream = (res_ref[:, n : n + block].astype(F32) + branch).astype(BF)
        stream_out[:, n : n + block] = stream
        wide = stream.astype(F32)
        squares = squares + jnp.sum(wide * wide, axis=1, keepdims=True)
    scale = lax.rsqrt(squares / weight.shape[1] + NORM_EPS)
    for n in range(0, weight.shape[1], 2 * block):
        cols = slice(n, n + 2 * block)
        normed = (stream_out[:, cols].astype(F32) * scale * gain_ref[:, cols]).astype(BF)
        normed_out[:, cols] = normed
        sent = jnp.dot(chosen, normed, preferred_element_type=F32).astype(BF)
        send_out[:, :, cols] = sent.reshape(experts, cap, 2 * block)


def post(info, parts, weights, turns, residual, gain, ids_t, experts, cap):
    rows, width = residual.shape
    vmem = pl.BlockSpec(memory_space=pltpu.VMEM)
    return pl.pallas_call(
        functools.partial(post_kernel, turns=turns, count=len(weights)),
        in_specs=[pl.BlockSpec(memory_space=pltpu.SMEM), vmem]
        + [pl.BlockSpec(memory_space=pltpu.HBM)] * len(weights)
        + [vmem] * 3,
        out_specs=[vmem] * 3,
        scratch_shapes=[
            pltpu.VMEM((rows, width), BF),
            pltpu.VMEM((width, width), BF),
            pltpu.SemaphoreType.DMA((len(weights),)),
        ],
        out_shape=[
            jax.ShapeDtypeStruct((rows, width), BF),
            jax.ShapeDtypeStruct((rows, width), BF),
            jax.ShapeDtypeStruct((experts, cap, width), BF),
        ],
        compiler_params=pltpu.CompilerParams(vmem_limit_bytes=40 * 1024 * 1024),
        name="post",
    )(info, parts, *weights, residual, gain, ids_t)


def expert_kernel(x_ref, gate_ref, up_ref, down_ref, out_ref):
    peers, cap, width = x_ref.shape
    x = x_ref[...].reshape(peers * cap, width)
    gate = jnp.dot(x, gate_ref[0], preferred_element_type=F32)
    up = jnp.dot(x, up_ref[0], preferred_element_type=F32)
    hidden = (gate / (1.0 + jnp.exp(-gate)) * up).astype(BF)
    out = jnp.dot(hidden, down_ref[0], preferred_element_type=F32).astype(BF)
    out_ref[...] = out.reshape(peers, cap, width)


def expert(arrived, gate, up, down, steps=4):
    peers, cap, width = arrived.shape
    rows = pl.BlockSpec((peers // steps, cap, width), lambda g: (g, 0, 0))
    whole = lambda g: (0, 0, 0)
    return pl.pallas_call(
        expert_kernel,
        grid=(steps,),
        in_specs=[
            rows,
            pl.BlockSpec(gate.shape, whole),
            pl.BlockSpec(up.shape, whole),
            pl.BlockSpec(down.shape, whole),
        ],
        out_specs=rows,
        out_shape=pltpu.HBM(arrived.shape, BF),
        compiler_params=pltpu.CompilerParams(
            dimension_semantics=("arbitrary",), vmem_limit_bytes=40 * 1024 * 1024
        ),
        name="expert",
    )(arrived, gate, up, down)


def finish_kernel(res_ref, base_ref, ids_ref, route_ref, out_ref, mix):
    rows = base_ref.shape[0]
    experts, cap, block = res_ref.shape
    slots = experts * cap

    @pl.when(pl.program_id(0) == 0)
    def _():
        route = route_ref[...]
        gates = route / jnp.sum(route, axis=1, keepdims=True) * ROUTED_SCALE
        expert = lax.broadcasted_iota(jnp.int32, (rows, experts), 1)
        named = jnp.zeros((rows, experts), F32)
        gate = jnp.zeros((rows, experts), F32)
        for k in range(TOPK):
            here = ids_ref[:, k : k + 1] == expert
            named = jnp.where(here, 1.0, named)
            gate = jnp.where(here, gates[:, k : k + 1], gate)
        earlier = (
            lax.broadcasted_iota(jnp.int32, (rows, rows), 1)
            < lax.broadcasted_iota(jnp.int32, (rows, rows), 0)
        ).astype(BF)
        rank = jnp.dot(earlier, named.astype(BF), preferred_element_type=F32)
        rank = jnp.where(named > 0.5, rank, 128.0)
        high = gate.astype(BF)
        low = (gate - high.astype(F32)).astype(BF)
        slot = lax.broadcasted_iota(jnp.int32, (experts, slots), 1)
        first = lax.broadcasted_iota(jnp.int32, (experts, slots), 0) * cap
        spread = ((slot >= first) & (slot < first + cap)).astype(BF)
        stacked = jnp.concatenate([rank.astype(BF), high, low], axis=0)
        wide = jnp.dot(stacked, spread, preferred_element_type=F32)
        place = (lax.broadcasted_iota(jnp.int32, (rows, slots), 1) % cap).astype(F32)
        chosen = wide[:rows] == place
        mix[:rows] = jnp.where(chosen, wide[rows : 2 * rows], 0.0).astype(BF)
        mix[rows:] = jnp.where(chosen, wide[2 * rows :], 0.0).astype(BF)

    results = res_ref[...].reshape(slots, block)
    routed = jnp.dot(mix[...], results, preferred_element_type=F32)
    out_ref[...] = (base_ref[...] + routed[:rows] + routed[rows:]).astype(BF)


def finish(results, base, ids, route):
    experts, cap, width = results.shape
    rows = base.shape[0]
    block = 512
    tiled = pl.BlockSpec((rows, block), lambda g: (0, g))
    fixed = pl.BlockSpec(ids.shape, lambda g: (0, 0))
    return pl.pallas_call(
        finish_kernel,
        grid=(width // block,),
        in_specs=[
            pl.BlockSpec((experts, cap, block), lambda g: (0, 0, g)),
            tiled,
            fixed,
            fixed,
        ],
        out_specs=tiled,
        scratch_shapes=[pltpu.VMEM((2 * rows, experts * cap), BF)],
        out_shape=jax.ShapeDtypeStruct(base.shape, BF),
        compiler_params=pltpu.CompilerParams(dimension_semantics=("arbitrary",)),
        name="finish",
    )(results, base, ids, route)


def local(
    residual,
    queries,
    key_rows,
    value_rows,
    forget_sums,
    out_weight,
    norm_gain,
    expert_ids,
    route_weights,
    expert_gate,
    expert_up,
    expert_down,
    shared_gate,
    shared_up,
    shared_down,
):
    z_count = lax.axis_size("z")
    y_count = lax.axis_size("y")
    z = lax.axis_index("z")
    y = lax.axis_index("y")
    rows = queries.shape[0]
    experts = z_count * y_count * 2
    cap = 2 * residual.shape[0] * TOPK // experts

    tps = lax.axis_size("tp")
    f_t = forget_sums.T
    kv_send = pack_keys(key_rows, value_rows, f_t)
    own = lax.all_to_all(kv_send, "c", split_axis=0, concat_axis=0)
    up_ring = [(i, (i + 1) % z_count) for i in range(z_count)]
    down_ring = [(i, (i - 1) % z_count) for i in range(z_count)]
    q_send = pack_queries(queries, f_t, own, y_count)
    q_all = lax.all_to_all(q_send, ("y", "c"), split_axis=0, concat_axis=0)
    core = lax.axis_index("c")
    half_rows = out_weight.shape[0] // 2
    mine = lax.dynamic_slice_in_dim(out_weight, core * half_rows, half_rows, 0)
    next_tp = [(i, (i + 1) % tps) for i in range(tps)]
    last_tp = [(i, (i - 1) % tps) for i in range(tps)]
    w_up = lax.ppermute(mine, "tp", next_tp)
    w_down = lax.ppermute(mine, "tp", last_tp)

    def swap(x):
        return lax.ppermute(x, "c", [(0, 1), (1, 0)])

    def up(block):
        return lax.ppermute(block, "z", up_ring)

    def down(block):
        return lax.ppermute(block, "z", down_ring)

    info = jnp.stack([2 * y * rows, z, lax.axis_index("tp"), core]).astype(jnp.int32)
    up1, down1 = up(own), down(own)
    up2, down2 = up(up1), down(down1)
    up3, down3 = up(up2), down(down2)
    state = attend(info, q_all, [own, up1, down1], (0, 1, -1), z_count, None, False)
    state, up3, down3, w_up = lax.optimization_barrier((state, up3, down3, w_up))
    up4 = up(up3)
    w_far = lax.ppermute(w_up, "tp", next_tp)
    state = attend(info, q_all, [up2, down2], (2, -2), z_count, state, False)
    state, w_down = lax.optimization_barrier((state, w_down))
    w_up2, w_down2 = swap(w_up), swap(w_down)
    sent = attend(info, q_all, [up3, down3, up4], (3, -3, 4), z_count, state, True)
    sent, w_far = lax.optimization_barrier((sent, w_far))
    w_far2 = swap(w_far)
    parts = lax.all_to_all(sent, ("y", "c", "tp"), split_axis=0, concat_axis=0)
    weights = [out_weight, w_up, w_up2, w_down, w_down2, w_far, w_far2]
    stream, normed, outgoing = post(
        info,
        parts,
        weights,
        (0, tps - 1, 1, 2),
        residual,
        norm_gain[None, :],
        expert_ids.T,
        experts,
        cap,
    )
    arrived = lax.all_to_all(outgoing, ("z", "y", "c"), split_axis=0, concat_axis=0)
    shared_hidden = (
        jax.nn.silu(jnp.dot(normed, shared_gate, preferred_element_type=F32))
        * jnp.dot(normed, shared_up, preferred_element_type=F32)
    ).astype(BF)
    base = stream.astype(F32) + jnp.dot(shared_hidden, shared_down, preferred_element_type=F32)
    processed = expert(arrived, expert_gate, expert_up, expert_down)
    returned = lax.all_to_all(
        processed, ("z", "y", "c"), split_axis=0, concat_axis=0
    )
    return finish(returned, base, expert_ids, route_weights)


def solution(mesh):
    sp = mesh.shape["sp"]
    tp = mesh.shape["tp"]
    grid = Mesh(mesh.devices.reshape(8, sp // 16, 2, tp), ("z", "y", "c", "tp"))
    seq = ("z", "y", "c")
    in_specs = (
        P((*seq, "tp"), None),
        P(seq, "tp"),
        P(seq, "tp"),
        P(seq, "tp"),
        P(seq, "tp"),
        P("tp", None),
        P(),
        P((*seq, "tp"), None),
        P((*seq, "tp"), None),
        P(seq, None, None),
        P(seq, None, None),
        P(seq, None, None),
        P(),
        P(),
        P(),
    )
    out_specs = P((*seq, "tp"), None)

    return jax.shard_map(local, mesh=grid, in_specs=in_specs, out_specs=out_specs, check_vma=False)
```

```python
import functools
import math

import jax
import jax.numpy as jnp
from jax import lax
from jax.experimental import pallas as pl
from jax.experimental.pallas import tpu as pltpu
from jax.sharding import Mesh, PartitionSpec as P

HEAD_DIM = 128
TOPK = 4
ROUTED_SCALE = 2.5
NORM_EPS = 1e-06
LOG2E = math.log2(math.e)
SCORE2 = HEAD_DIM**-0.5 * LOG2E
LOW = -1e30
TAIL = 8

BF = jnp.bfloat16
F32 = jnp.float32


def pieces(row):
    high = row.astype(BF)
    rest = row - high.astype(F32)
    mid = rest.astype(BF)
    low = (rest - mid.astype(F32)).astype(BF)
    return [high.astype(F32), mid.astype(F32), low.astype(F32)]


def tail_block(rows, width):
    parts = [piece for row in rows for piece in pieces(row)]
    parts.append(jnp.zeros((TAIL - len(parts), width), F32))
    return jnp.concatenate(parts, axis=0).astype(BF)


def row_of(tail, j):
    return tail[3 * j : 3 * j + 1] + tail[3 * j + 1 : 3 * j + 2] + tail[3 * j + 2 : 3 * j + 3]


def pack_keys_kernel(k_ref, v_ref, f_ref, out):
    rows = k_ref.shape[0]
    for c in range(2):
        out[c, :rows, :HEAD_DIM] = k_ref[:, c * HEAD_DIM : (c + 1) * HEAD_DIM]
        out[c, :rows, HEAD_DIM:] = v_ref[:, c * HEAD_DIM : (c + 1) * HEAD_DIM]
        out[c, rows:, :] = tail_block([f_ref[2 * c : 2 * c + 1, :], f_ref[2 * c + 1 : 2 * c + 2, :]], rows)


def pack_queries_kernel(q_ref, f_ref, _, out):
    rows = q_ref.shape[0]
    for c in range(2):
        tail = tail_block([f_ref[2 * c : 2 * c + 1, :], f_ref[2 * c + 1 : 2 * c + 2, :]], rows)
        part = q_ref[:, c * 2 * HEAD_DIM : (c + 1) * 2 * HEAD_DIM]
        for y in range(out.shape[0] // 2):
            out[2 * y + c, :rows, :] = part
            out[2 * y + c, rows:, :] = tail


def pack_keys(k, v, f_t):
    return pl.pallas_call(
        pack_keys_kernel,
        out_shape=pltpu.HBM((2, k.shape[0] + TAIL, 2 * HEAD_DIM), BF),
        name="pack_keys",
    )(k, v, f_t)


def pack_queries(q, f_t, after, ys):
    return pl.pallas_call(
        pack_queries_kernel,
        in_specs=[pl.BlockSpec(), pl.BlockSpec(), pl.BlockSpec(memory_space=pl.ANY)],
        out_shape=pltpu.HBM((2 * ys, q.shape[0] + TAIL, 2 * HEAD_DIM), BF),
        name="pack_queries",
    )(q, f_t, after)


def attend_kernel(info, *refs, steps, z_count, first, last, tiles, rows):
    blocks, own = len(steps), 0 in steps
    q_ref = refs[0]
    kv_refs = refs[1 : 1 + blocks]
    at = 1 + blocks
    if not first:
        acc_in, stat_in = refs[at], refs[at + 1]
        at += 2
    if last:
        (o_out,) = refs[at : at + 1]
    else:
        acc_out, stat_out = refs[at : at + 2]
    first_tail = q_ref[0, rows:, :].astype(F32)
    keys, values, biases = [], [], []
    ones = jnp.ones((rows, HEAD_DIM), BF)
    for b, s in enumerate(steps):
        valid = info[1] >= s if s >= 0 else info[1] - s >= z_count
        for c in range(2):
            keys.append(kv_refs[b].at[c, pl.ds(0, rows), pl.ds(0, HEAD_DIM)])
            values.append(kv_refs[b].at[c, pl.ds(0, rows), pl.ds(HEAD_DIM, HEAD_DIM)])
            tail = kv_refs[b][c, rows:, :].astype(F32)
            pair = []
            for j in range(2):
                bias = (row_of(first_tail, j)[:, :1] - row_of(tail, j)) * LOG2E
                pair.append(jnp.where(valid, bias, -jnp.inf))
            biases.append(pair)

    def score_tiles(i):
        both = jnp.concatenate(
            [q_ref[i, pl.ds(0, rows), pl.ds(j * HEAD_DIM, HEAD_DIM)] for j in range(2)], axis=0
        )
        found = [[], []]
        for u in range(2 * blocks):
            raw = lax.dot_general(
                both, keys[u][...], (((1,), (1,)), ((), ())), preferred_element_type=F32
            )
            for j in range(2):
                score = raw[j * rows : (j + 1) * rows] * SCORE2 + biases[u][j]
                if own and u < 2:
                    q_pos = i * rows + lax.broadcasted_iota(
                        jnp.int32, (rows, rows), 0
                    )
                    k_pos = info[0] + u * rows + lax.broadcasted_iota(jnp.int32, (rows, rows), 1)
                    score = jnp.where(q_pos >= k_pos, score, -jnp.inf)
                found[j].append(score)
        return found

    def absorb(i, scores):
        maxes, olds = [], []
        for j in range(2):
            top = scores[j][0]
            for score in scores[j][1:]:
                top = jnp.maximum(top, score)
            row_max = jnp.max(top, axis=1, keepdims=True)
            cols = pl.ds(j * HEAD_DIM, HEAD_DIM)
            old_max = jnp.full((rows, HEAD_DIM), LOW, F32) if first else stat_in[i, :, cols]
            olds.append(old_max)
            maxes.append(jnp.maximum(row_max, old_max))
        total = None
        wide = rows // HEAD_DIM
        for u in range(2 * blocks):
            weights = jnp.concatenate(
                [
                    jnp.exp2(scores[j][u] - jnp.concatenate([maxes[j]] * wide, axis=1)).astype(BF)
                    for j in range(2)
                ],
                axis=0,
            )
            value = jnp.concatenate([values[u][...], ones], axis=1)
            part = jnp.dot(weights, value, preferred_element_type=F32)
            total = part if total is None else total + part
        lse_rows = []
        for j in range(2):
            cols = pl.ds(j * HEAD_DIM, HEAD_DIM)
            weighted = total[j * rows : (j + 1) * rows, :HEAD_DIM]
            row_sum = total[j * rows : (j + 1) * rows, HEAD_DIM:]
            if not first:
                factor = jnp.exp2(olds[j] - maxes[j])
                sums = pl.ds((2 + j) * HEAD_DIM, HEAD_DIM)
                weighted = weighted + acc_in[i, :, cols] * factor
                row_sum = row_sum + acc_in[i, :, sums] * factor
            if last:
                some = row_sum > 0.0
                row_sum = jnp.where(some, row_sum, 1.0)
                mixed = weighted * (1.0 / row_sum)
                per = rows // 4
                for p in range(4):
                    o_out[4 * i + p, pl.ds(0, per), cols] = mixed[p * per : (p + 1) * per].astype(BF)
                lse = jnp.where(some, maxes[j] + jnp.log2(row_sum), LOW)
                flat = []
                eye = lax.broadcasted_iota(jnp.int32, (HEAD_DIM, HEAD_DIM), 0) == (
                    lax.broadcasted_iota(jnp.int32, (HEAD_DIM, HEAD_DIM), 1)
                )
                for at in range(0, rows, HEAD_DIM):
                    flat.append(
                        jnp.sum(jnp.where(eye, lse[at : at + HEAD_DIM], 0.0), axis=0, keepdims=True)
                    )
                lse_rows.append(jnp.concatenate(flat, axis=1))
            else:
                acc_out[i, :, cols] = weighted
                acc_out[i, :, pl.ds((2 + j) * HEAD_DIM, HEAD_DIM)] = row_sum
                stat_out[i, :, cols] = maxes[j]
        if last:
            tail = tail_block(lse_rows, rows)
            for p in range(4):
                o_out[4 * i + p, pl.ds(rows // 4, TAIL), :] = tail

    def some_tiles(step, _):
        pending = score_tiles(step * tiles)
        for n in range(tiles):
            i = step * tiles + n
            following = score_tiles(i + 1) if n + 1 < tiles else None
            absorb(i, pending)
            pending = following
        return 0

    lax.fori_loop(0, q_ref.shape[0] // tiles, some_tiles, 0)


def attend(info, q_all, kvs, steps, z_count, state, last, tiles=4):
    count, padded, width = q_all.shape
    rows = padded - TAIL
    first = state is None
    blocks = len(kvs)
    vmem = pl.BlockSpec(memory_space=pltpu.VMEM)
    operands = [q_all, *kvs]
    aliases = {}
    if not first:
        operands += list(state)
        if not last:
            aliases = {len(operands) - 1: 0, len(operands): 1}
    if last:
        out_shape = jax.ShapeDtypeStruct((4 * count, rows // 4 + TAIL, width), BF)
    else:
        out_shape = [
            jax.ShapeDtypeStruct((count, rows, 2 * width), F32),
            jax.ShapeDtypeStruct((count, rows, width), F32),
        ]
    scores = count * rows * 2 * blocks * 2 * rows
    return pl.pallas_call(
        functools.partial(
            attend_kernel, steps=steps, z_count=z_count, first=first, last=last, tiles=tiles, rows=rows
        ),
        in_specs=[pl.BlockSpec(memory_space=pltpu.SMEM)] + [vmem] * len(operands),
        out_specs=vmem if last else [vmem, vmem],
        out_shape=out_shape,
        input_output_aliases=aliases,
        cost_estimate=pl.CostEstimate(
            flops=scores * 768, transcendentals=scores, bytes_accessed=6_000_000
        ),
        compiler_params=pltpu.CompilerParams(vmem_limit_bytes=24 * 1024 * 1024),
    )(info, *operands)


def post_kernel(info, part_ref, *refs, tps):
    w_refs = refs[:tps]
    res_ref, gain_ref, ids_ref, stream_out, normed_out, send_out, att, weight, sems = refs[tps:]
    sources = part_ref.shape[0]
    own_rows = res_ref.shape[0]
    width = part_ref.shape[2]
    groups = 2 * tps
    ys = sources // groups
    copies = []
    at = 0
    for n, w_ref in enumerate(w_refs):
        size = w_ref.shape[0]
        copies.append(pltpu.make_async_copy(w_ref, weight.at[pl.ds(at, size)], sems.at[n]))
        copies[-1].start()
        at += size

    pick = lax.broadcasted_iota(jnp.int32, (own_rows, width), 1) == (
        info[2] * own_rows + lax.broadcasted_iota(jnp.int32, (own_rows, width), 0)
    )
    near = 2 * info[3] - 1
    for s, turn in enumerate((0, near, -near, 2)):
        tp = (info[2] + turn + tps) % tps
        for core in range(2):
            col = (2 * s + core) * width
            index = core * tps + tp
            tails = [part_ref[y * groups + index, own_rows:, :].astype(F32) for y in range(ys)]
            for j in range(2):
                sums = []
                for y in range(ys):
                    row = row_of(tails[y], j)
                    sums.append(jnp.sum(jnp.where(pick, row, 0.0), axis=1, keepdims=True))
                top = sums[0]
                for one in sums[1:]:
                    top = jnp.maximum(top, one)
                weights = [jnp.exp2(one - top) for one in sums]
                total = weights[0]
                for w in weights[1:]:
                    total = total + w
                inverse = 1.0 / total
                mixed = None
                for y in range(ys):
                    part = part_ref[
                        y * groups + index, pl.ds(0, own_rows), pl.ds(j * HEAD_DIM, HEAD_DIM)
                    ].astype(F32) * (weights[y] * inverse)
                    mixed = part if mixed is None else mixed + part
                att[:, pl.ds(col + j * HEAD_DIM, HEAD_DIM)] = mixed.astype(BF)

    experts = send_out.shape[0]
    cap = send_out.shape[1]
    expert = lax.broadcasted_iota(jnp.int32, (experts, own_rows), 0)
    named = jnp.zeros((experts, own_rows), F32)
    for k in range(TOPK):
        named = jnp.where(ids_ref[k : k + 1, :] == expert, 1.0, named)
    earlier = (
        lax.broadcasted_iota(jnp.int32, (own_rows, own_rows), 0)
        < lax.broadcasted_iota(jnp.int32, (own_rows, own_rows), 1)
    ).astype(BF)
    rank = jnp.dot(named.astype(BF), earlier, preferred_element_type=F32)
    rank = jnp.where(named > 0.5, rank, -1.0)
    slot = lax.broadcasted_iota(jnp.int32, (experts, cap, own_rows), 1).astype(F32)
    chosen = (rank[:, None, :] == slot).astype(F32).reshape(experts * cap, own_rows).astype(BF)

    for copy in copies:
        copy.wait()
    block = 256
    squares = jnp.zeros((own_rows, 1), F32)
    for n in range(0, weight.shape[1], block):
        branch = jnp.dot(att[...], weight[:, n : n + block], preferred_element_type=F32)
        stream = (res_ref[:, n : n + block].astype(F32) + branch).astype(BF)
        stream_out[:, n : n + block] = stream
        wide = stream.astype(F32)
        squares = squares + jnp.sum(wide * wide, axis=1, keepdims=True)
    scale = lax.rsqrt(squares / weight.shape[1] + NORM_EPS)
    for n in range(0, weight.shape[1], 2 * block):
        cols = slice(n, n + 2 * block)
        normed = (stream_out[:, cols].astype(F32) * scale * gain_ref[:, cols]).astype(BF)
        normed_out[:, cols] = normed
        sent = jnp.dot(chosen, normed, preferred_element_type=F32).astype(BF)
        send_out[:, :, cols] = sent.reshape(experts, cap, 2 * block)


def post(info, parts, weights, residual, gain, ids_t, experts, cap):
    rows, width = residual.shape
    vmem = pl.BlockSpec(memory_space=pltpu.VMEM)
    return pl.pallas_call(
        functools.partial(post_kernel, tps=len(weights)),
        in_specs=[pl.BlockSpec(memory_space=pltpu.SMEM), vmem]
        + [pl.BlockSpec(memory_space=pltpu.HBM)] * len(weights)
        + [vmem] * 3,
        out_specs=[vmem] * 3,
        scratch_shapes=[
            pltpu.VMEM((rows, width), BF),
            pltpu.VMEM((width, width), BF),
            pltpu.SemaphoreType.DMA((len(weights),)),
        ],
        out_shape=[
            jax.ShapeDtypeStruct((rows, width), BF),
            jax.ShapeDtypeStruct((rows, width), BF),
            jax.ShapeDtypeStruct((experts, cap, width), BF),
        ],
        compiler_params=pltpu.CompilerParams(vmem_limit_bytes=56 * 1024 * 1024),
        name="post",
    )(info, parts, *weights, residual, gain, ids_t)


def expert_kernel(x_ref, gate_ref, up_ref, down_ref, out_ref):
    peers, cap, width = x_ref.shape
    x = x_ref[...].reshape(peers * cap, width)
    gate = jnp.dot(x, gate_ref[0], preferred_element_type=F32)
    up = jnp.dot(x, up_ref[0], preferred_element_type=F32)
    hidden = (gate / (1.0 + jnp.exp(-gate)) * up).astype(BF)
    out = jnp.dot(hidden, down_ref[0], preferred_element_type=F32).astype(BF)
    out_ref[...] = out.reshape(peers, cap, width)


def expert(arrived, gate, up, down, steps=4):
    peers, cap, width = arrived.shape
    rows = pl.BlockSpec((peers // steps, cap, width), lambda g: (g, 0, 0))
    whole = lambda g: (0, 0, 0)
    return pl.pallas_call(
        expert_kernel,
        grid=(steps,),
        in_specs=[
            rows,
            pl.BlockSpec(gate.shape, whole),
            pl.BlockSpec(up.shape, whole),
            pl.BlockSpec(down.shape, whole),
        ],
        out_specs=rows,
        out_shape=pltpu.HBM(arrived.shape, BF),
        compiler_params=pltpu.CompilerParams(
            dimension_semantics=("arbitrary",), vmem_limit_bytes=40 * 1024 * 1024
        ),
        name="expert",
    )(arrived, gate, up, down)


def mix_kernel(ids_ref, route_ref, mix, *, cap):
    rows = ids_ref.shape[0]
    slots = mix.shape[1]
    experts = slots // cap
    route = route_ref[...]
    gates = route / jnp.sum(route, axis=1, keepdims=True) * ROUTED_SCALE
    expert = lax.broadcasted_iota(jnp.int32, (rows, experts), 1)
    named = jnp.zeros((rows, experts), F32)
    gate = jnp.zeros((rows, experts), F32)
    for k in range(TOPK):
        here = ids_ref[:, k : k + 1] == expert
        named = jnp.where(here, 1.0, named)
        gate = jnp.where(here, gates[:, k : k + 1], gate)
    earlier = (
        lax.broadcasted_iota(jnp.int32, (rows, rows), 1)
        < lax.broadcasted_iota(jnp.int32, (rows, rows), 0)
    ).astype(BF)
    rank = jnp.dot(earlier, named.astype(BF), preferred_element_type=F32)
    rank = jnp.where(named > 0.5, rank, 128.0)
    high = gate.astype(BF)
    low = (gate - high.astype(F32)).astype(BF)
    slot = lax.broadcasted_iota(jnp.int32, (experts, slots), 1)
    first = lax.broadcasted_iota(jnp.int32, (experts, slots), 0) * cap
    spread = ((slot >= first) & (slot < first + cap)).astype(BF)
    stacked = jnp.concatenate([rank.astype(BF), high, low], axis=0)
    wide = jnp.dot(stacked, spread, preferred_element_type=F32)
    place = (lax.broadcasted_iota(jnp.int32, (rows, slots), 1) % cap).astype(F32)
    chosen = wide[:rows] == place
    mix[:rows] = jnp.where(chosen, wide[rows : 2 * rows], 0.0).astype(BF)
    mix[rows:] = jnp.where(chosen, wide[2 * rows :], 0.0).astype(BF)


def mixing(ids, route, experts, cap):
    return pl.pallas_call(
        functools.partial(mix_kernel, cap=cap),
        out_shape=jax.ShapeDtypeStruct((2 * ids.shape[0], experts * cap), BF),
        name="mixing",
    )(ids, route)


def finish_kernel(res_ref, base_ref, mix_ref, out_ref):
    rows = base_ref.shape[0]
    experts, cap, block = res_ref.shape
    results = res_ref[...].reshape(experts * cap, block)
    routed = jnp.dot(mix_ref[...], results, preferred_element_type=F32)
    out_ref[...] = (base_ref[...] + routed[:rows] + routed[rows:]).astype(BF)


def finish(results, base, mix):
    experts, cap, width = results.shape
    rows = base.shape[0]
    block = 512
    tiled = pl.BlockSpec((rows, block), lambda g: (0, g))
    return pl.pallas_call(
        finish_kernel,
        grid=(width // block,),
        in_specs=[
            pl.BlockSpec((experts, cap, block), lambda g: (0, 0, g)),
            tiled,
            pl.BlockSpec(mix.shape, lambda g: (0, 0)),
        ],
        out_specs=tiled,
        out_shape=jax.ShapeDtypeStruct(base.shape, BF),
        compiler_params=pltpu.CompilerParams(dimension_semantics=("arbitrary",)),
        name="finish",
    )(results, base, mix)


def local(
    residual,
    queries,
    key_rows,
    value_rows,
    forget_sums,
    out_weight,
    norm_gain,
    expert_ids,
    route_weights,
    expert_gate,
    expert_up,
    expert_down,
    shared_gate,
    shared_up,
    shared_down,
):
    z_count = lax.axis_size("z")
    y_count = lax.axis_size("y")
    z = lax.axis_index("z")
    y = lax.axis_index("y")
    rows = queries.shape[0]
    experts = z_count * y_count * 2
    cap = 2 * residual.shape[0] * TOPK // experts

    tps = lax.axis_size("tp")
    f_t = forget_sums.T
    kv_send = pack_keys(key_rows, value_rows, f_t)
    own = lax.all_to_all(kv_send, "c", split_axis=0, concat_axis=0)
    up_ring = [(i, (i + 1) % z_count) for i in range(z_count)]
    down_ring = [(i, (i - 1) % z_count) for i in range(z_count)]
    q_send = pack_queries(queries, f_t, own, y_count)
    q_all = lax.all_to_all(q_send, ("y", "c"), split_axis=0, concat_axis=0)
    core = lax.axis_index("c")
    turn = [(i, (i + 1) % tps) for i in range(tps)]
    turn += [(tps + i, tps + (i - 1) % tps) for i in range(tps)]
    w_near = lax.ppermute(out_weight, ("c", "tp"), turn)

    def up(block):
        return lax.ppermute(block, "z", up_ring)

    def down(block):
        return lax.ppermute(block, "z", down_ring)

    info = jnp.stack([2 * y * rows, z, lax.axis_index("tp"), core]).astype(jnp.int32)
    up1, down1 = up(own), down(own)
    up2, down2 = up(up1), down(down1)
    up3, down3 = up(up2), down(down2)
    state = attend(info, q_all, [own, up1, down1], (0, 1, -1), z_count, None, False)
    state, up3, down3, _ = lax.optimization_barrier((state, up3, down3, w_near))
    up4 = up(up3)
    w_far = lax.ppermute(w_near, ("c", "tp"), turn)
    state = attend(info, q_all, [up2, down2], (2, -2), z_count, state, False)
    w_other = lax.ppermute(w_near, "c", [(0, 1), (1, 0)])
    sent = attend(info, q_all, [up3, down3, up4], (3, -3, 4), z_count, state, True)
    parts = lax.all_to_all(sent, ("y", "c", "tp"), split_axis=0, concat_axis=0)
    weights = [out_weight, w_near, w_other, w_far]
    stream, normed, outgoing = post(
        info,
        parts,
        weights,
        residual,
        norm_gain[None, :],
        expert_ids.T,
        experts,
        cap,
    )
    arrived = lax.all_to_all(outgoing, ("z", "y", "c"), split_axis=0, concat_axis=0)
    shared_hidden = (
        jax.nn.silu(jnp.dot(normed, shared_gate, preferred_element_type=F32))
        * jnp.dot(normed, shared_up, preferred_element_type=F32)
    ).astype(BF)
    base = stream.astype(F32) + jnp.dot(shared_hidden, shared_down, preferred_element_type=F32)
    processed = expert(arrived, expert_gate, expert_up, expert_down)
    returned = lax.all_to_all(
        processed, ("z", "y", "c"), split_axis=0, concat_axis=0
    )
    mix = mixing(expert_ids, route_weights, experts, cap)
    return finish(returned, base, mix)


def solution(mesh):
    sp = mesh.shape["sp"]
    tp = mesh.shape["tp"]
    grid = Mesh(mesh.devices.reshape(8, sp // 16, 2, tp), ("z", "y", "c", "tp"))
    seq = ("z", "y", "c")
    in_specs = (
        P((*seq, "tp"), None),
        P(seq, "tp"),
        P(seq, "tp"),
        P(seq, "tp"),
        P(seq, "tp"),
        P("tp", None),
        P(),
        P((*seq, "tp"), None),
        P((*seq, "tp"), None),
        P(seq, None, None),
        P(seq, None, None),
        P(seq, None, None),
        P(),
        P(),
        P(),
    )
    out_specs = P((*seq, "tp"), None)

    return jax.shard_map(local, mesh=grid, in_specs=in_specs, out_specs=out_specs, check_vma=False)
```

```python
import functools
import math

import jax
import jax.numpy as jnp
from jax import lax
from jax.experimental import pallas as pl
from jax.experimental.pallas import tpu as pltpu
from jax.sharding import Mesh, PartitionSpec as P

HEAD_DIM = 128
TOPK = 4
ROUTED_SCALE = 2.5
NORM_EPS = 1e-06
LOG2E = math.log2(math.e)
SCORE2 = HEAD_DIM**-0.5 * LOG2E
LOW = -1e30
TAIL = 8

BF = jnp.bfloat16
F32 = jnp.float32


def pieces(row):
    high = row.astype(BF)
    rest = row - high.astype(F32)
    mid = rest.astype(BF)
    low = (rest - mid.astype(F32)).astype(BF)
    return [high.astype(F32), mid.astype(F32), low.astype(F32)]


def tail_block(rows, width):
    parts = [piece for row in rows for piece in pieces(row)]
    parts.append(jnp.zeros((TAIL - len(parts), width), F32))
    return jnp.concatenate(parts, axis=0).astype(BF)


def row_of(tail, j):
    return tail[3 * j : 3 * j + 1] + tail[3 * j + 1 : 3 * j + 2] + tail[3 * j + 2 : 3 * j + 3]


def pack_keys_kernel(info, k_ref, v_ref, f_ref, mine, other):
    rows = k_ref.shape[0]
    for out, c in ((mine, info[3]), (other, 1 - info[3])):
        cols = pl.ds(pl.multiple_of(c * HEAD_DIM, HEAD_DIM), HEAD_DIM)
        out[:rows, :HEAD_DIM] = k_ref[:, cols]
        out[:rows, HEAD_DIM:] = v_ref[:, cols]
        out[rows:, :] = tail_block([f_ref[pl.ds(2 * c + j, 1), :] for j in range(2)], rows)


def pack_queries_kernel(q_ref, f_ref, _, out):
    rows = q_ref.shape[0]
    for c in range(2):
        tail = tail_block([f_ref[2 * c : 2 * c + 1, :], f_ref[2 * c + 1 : 2 * c + 2, :]], rows)
        part = q_ref[:, c * 2 * HEAD_DIM : (c + 1) * 2 * HEAD_DIM]
        for y in range(out.shape[0] // 2):
            out[2 * y + c, :rows, :] = part
            out[2 * y + c, rows:, :] = tail


def pack_keys(info, k, v, f_t):
    shape = (k.shape[0] + TAIL, 2 * HEAD_DIM)
    vmem = pl.BlockSpec(memory_space=pltpu.VMEM)
    return pl.pallas_call(
        pack_keys_kernel,
        in_specs=[pl.BlockSpec(memory_space=pltpu.SMEM)] + [vmem] * 3,
        out_shape=(pltpu.HBM(shape, BF), pltpu.HBM(shape, BF)),
        name="pack_keys",
    )(info, k, v, f_t)


def pack_queries(q, f_t, after, ys):
    return pl.pallas_call(
        pack_queries_kernel,
        in_specs=[pl.BlockSpec(), pl.BlockSpec(), pl.BlockSpec(memory_space=pl.ANY)],
        out_shape=pltpu.HBM((2 * ys, q.shape[0] + TAIL, 2 * HEAD_DIM), BF),
        name="pack_queries",
    )(q, f_t, after)


def attend_kernel(info, *refs, steps, z_count, first, last, tiles, rows):
    blocks, own = len(steps), 0 in steps
    q_ref = refs[0]
    kv_refs = refs[1 : 1 + blocks]
    at = 1 + blocks
    if not first:
        acc_in, stat_in = refs[at], refs[at + 1]
        at += 2
    if last:
        (o_out,) = refs[at : at + 1]
    else:
        acc_out, stat_out = refs[at : at + 2]
    first_tail = q_ref[0, rows:, :].astype(F32)
    keys, values, biases = [], [], []
    ones = jnp.ones((rows, HEAD_DIM), BF)
    for b, s in enumerate(steps):
        valid = info[1] >= s if s >= 0 else info[1] - s >= z_count
        for c in range(2):
            keys.append(kv_refs[b].at[c, pl.ds(0, rows), pl.ds(0, HEAD_DIM)])
            values.append(kv_refs[b].at[c, pl.ds(0, rows), pl.ds(HEAD_DIM, HEAD_DIM)])
            tail = kv_refs[b][c, rows:, :].astype(F32)
            pair = []
            for j in range(2):
                bias = (row_of(first_tail, j)[:, :1] - row_of(tail, j)) * LOG2E
                pair.append(jnp.where(valid, bias, -jnp.inf))
            biases.append(pair)

    def score_tiles(i):
        both = jnp.concatenate(
            [q_ref[i, pl.ds(0, rows), pl.ds(j * HEAD_DIM, HEAD_DIM)] for j in range(2)], axis=0
        )
        found = [[], []]
        for u in range(2 * blocks):
            raw = lax.dot_general(
                both, keys[u][...], (((1,), (1,)), ((), ())), preferred_element_type=F32
            )
            for j in range(2):
                score = raw[j * rows : (j + 1) * rows] * SCORE2 + biases[u][j]
                if own and u < 2:
                    q_pos = i * rows + lax.broadcasted_iota(
                        jnp.int32, (rows, rows), 0
                    )
                    k_pos = info[0] + (u ^ info[3]) * rows + lax.broadcasted_iota(jnp.int32, (rows, rows), 1)
                    score = jnp.where(q_pos >= k_pos, score, -jnp.inf)
                found[j].append(score)
        return found

    def absorb(i, scores):
        maxes, olds = [], []
        for j in range(2):
            top = scores[j][0]
            for score in scores[j][1:]:
                top = jnp.maximum(top, score)
            row_max = jnp.max(top, axis=1, keepdims=True)
            cols = pl.ds(j * HEAD_DIM, HEAD_DIM)
            old_max = jnp.full((rows, HEAD_DIM), LOW, F32) if first else stat_in[i, :, cols]
            olds.append(old_max)
            maxes.append(jnp.maximum(row_max, old_max))
        total = None
        wide = rows // HEAD_DIM
        for u in range(2 * blocks):
            weights = jnp.concatenate(
                [
                    jnp.exp2(scores[j][u] - jnp.concatenate([maxes[j]] * wide, axis=1)).astype(BF)
                    for j in range(2)
                ],
                axis=0,
            )
            value = jnp.concatenate([values[u][...], ones], axis=1)
            part = jnp.dot(weights, value, preferred_element_type=F32)
            total = part if total is None else total + part
        lse_rows = []
        for j in range(2):
            cols = pl.ds(j * HEAD_DIM, HEAD_DIM)
            weighted = total[j * rows : (j + 1) * rows, :HEAD_DIM]
            row_sum = total[j * rows : (j + 1) * rows, HEAD_DIM:]
            if not first:
                factor = jnp.exp2(olds[j] - maxes[j])
                sums = pl.ds((2 + j) * HEAD_DIM, HEAD_DIM)
                weighted = weighted + acc_in[i, :, cols] * factor
                row_sum = row_sum + acc_in[i, :, sums] * factor
            if last:
                some = row_sum > 0.0
                row_sum = jnp.where(some, row_sum, 1.0)
                mixed = weighted * (1.0 / row_sum)
                per = rows // 4
                for p in range(4):
                    o_out[4 * i + p, pl.ds(0, per), cols] = mixed[p * per : (p + 1) * per].astype(BF)
                lse = jnp.where(some, maxes[j] + jnp.log2(row_sum), LOW)
                flat = []
                eye = lax.broadcasted_iota(jnp.int32, (HEAD_DIM, HEAD_DIM), 0) == (
                    lax.broadcasted_iota(jnp.int32, (HEAD_DIM, HEAD_DIM), 1)
                )
                for at in range(0, rows, HEAD_DIM):
                    flat.append(
                        jnp.sum(jnp.where(eye, lse[at : at + HEAD_DIM], 0.0), axis=0, keepdims=True)
                    )
                lse_rows.append(jnp.concatenate(flat, axis=1))
            else:
                acc_out[i, :, cols] = weighted
                acc_out[i, :, pl.ds((2 + j) * HEAD_DIM, HEAD_DIM)] = row_sum
                stat_out[i, :, cols] = maxes[j]
        if last:
            tail = tail_block(lse_rows, rows)
            for p in range(4):
                o_out[4 * i + p, pl.ds(rows // 4, TAIL), :] = tail

    def some_tiles(step, _):
        pending = score_tiles(step * tiles)
        for n in range(tiles):
            i = step * tiles + n
            following = score_tiles(i + 1) if n + 1 < tiles else None
            absorb(i, pending)
            pending = following
        return 0

    lax.fori_loop(0, q_ref.shape[0] // tiles, some_tiles, 0)


def attend(info, q_all, kvs, steps, z_count, state, last, tiles=4):
    count, padded, width = q_all.shape
    rows = padded - TAIL
    first = state is None
    blocks = len(kvs)
    vmem = pl.BlockSpec(memory_space=pltpu.VMEM)
    operands = [q_all, *kvs]
    aliases = {}
    if not first:
        operands += list(state)
        if not last:
            aliases = {len(operands) - 1: 0, len(operands): 1}
    if last:
        out_shape = jax.ShapeDtypeStruct((4 * count, rows // 4 + TAIL, width), BF)
    else:
        out_shape = [
            jax.ShapeDtypeStruct((count, rows, 2 * width), F32),
            jax.ShapeDtypeStruct((count, rows, width), F32),
        ]
    scores = count * rows * 2 * blocks * 2 * rows
    return pl.pallas_call(
        functools.partial(
            attend_kernel, steps=steps, z_count=z_count, first=first, last=last, tiles=tiles, rows=rows
        ),
        in_specs=[pl.BlockSpec(memory_space=pltpu.SMEM)] + [vmem] * len(operands),
        out_specs=vmem if last else [vmem, vmem],
        out_shape=out_shape,
        input_output_aliases=aliases,
        cost_estimate=pl.CostEstimate(
            flops=scores * 768, transcendentals=scores, bytes_accessed=6_000_000
        ),
        compiler_params=pltpu.CompilerParams(vmem_limit_bytes=24 * 1024 * 1024),
    )(info, *operands)


def post_kernel(info, part_ref, *refs, tps):
    w_refs = refs[:tps]
    res_ref, gain_ref, ids_ref, stream_out, normed_out, send_out, total_ref, weight, share, sems = refs[tps:]
    sources = part_ref.shape[0]
    own_rows = res_ref.shape[0]
    width = part_ref.shape[2]
    groups = 2 * tps
    ys = sources // groups
    copies = []
    at = 0
    for n, w_ref in enumerate(w_refs):
        size = w_ref.shape[0]
        copies.append(pltpu.make_async_copy(w_ref, weight.at[pl.ds(at, size)], sems.at[n]))
        copies[-1].start()
        at += size

    pick = lax.broadcasted_iota(jnp.int32, (own_rows, width), 1) == (
        info[2] * own_rows + lax.broadcasted_iota(jnp.int32, (own_rows, width), 0)
    )
    tails = part_ref[:, own_rows:, :].reshape(sources * TAIL, width)
    pieces_t = lax.dot_general(
        pick.astype(F32).astype(BF), tails, (((1,), (1,)), ((), ())), preferred_element_type=F32
    )
    last = pieces_t.shape[1]
    lses = pieces_t + pltpu.roll(pieces_t, last - 1, 1) + pltpu.roll(pieces_t, last - 2, 1)
    span = last // ys
    lses = [lses[:, y * span : (y + 1) * span] for y in range(ys)]
    top = lses[0]
    for one in lses[1:]:
        top = jnp.maximum(top, one)
    shares = [jnp.exp2(one - top) for one in lses]
    total = shares[0]
    for one in shares[1:]:
        total = total + one
    inverse = 1.0 / total
    shares = [one * inverse for one in shares]
    spare = jnp.zeros((own_rows, HEAD_DIM - 2 * ys), F32)
    for index in range(groups):
        columns = [
            shares[y][:, TAIL * index + 3 * j : TAIL * index + 3 * j + 1]
            for y in range(ys)
            for j in range(2)
        ]
        share[index] = jnp.concatenate([*columns, spare], axis=1)
    near = 2 * info[3] - 1
    turns = [(info[2] + turn + tps) % tps for turn in (0, near, -near, 2)]
    block = 2 * width
    quarter = weight.shape[0] // tps
    for s, tp in enumerate(turns):
        merged = []
        for core in range(2):
            index = core * tps + tp
            for j in range(2):
                mixed = None
                for y in range(ys):
                    part = part_ref[
                        y * groups + index, pl.ds(0, own_rows), pl.ds(j * HEAD_DIM, HEAD_DIM)
                    ].astype(F32) * share[index, :, y * 2 + j : y * 2 + j + 1]
                    mixed = part if mixed is None else mixed + part
                merged.append(mixed.astype(BF))
        attended = jnp.concatenate(merged, axis=1)
        copies[s].wait()
        for n in range(0, weight.shape[1], block):
            product = jnp.dot(
                attended,
                weight[s * quarter : (s + 1) * quarter, n : n + block],
                preferred_element_type=F32,
            )
            total_ref[:, n : n + block] = product if s == 0 else total_ref[:, n : n + block] + product

    experts = send_out.shape[0]
    cap = send_out.shape[1]
    expert = lax.broadcasted_iota(jnp.int32, (experts, own_rows), 0)
    named = jnp.zeros((experts, own_rows), F32)
    for k in range(TOPK):
        named = jnp.where(ids_ref[k : k + 1, :] == expert, 1.0, named)
    earlier = (
        lax.broadcasted_iota(jnp.int32, (own_rows, own_rows), 0)
        < lax.broadcasted_iota(jnp.int32, (own_rows, own_rows), 1)
    ).astype(BF)
    rank = jnp.dot(named.astype(BF), earlier, preferred_element_type=F32)
    rank = jnp.where(named > 0.5, rank, -1.0)
    slot = lax.broadcasted_iota(jnp.int32, (experts, cap, own_rows), 1).astype(F32)
    chosen = (rank[:, None, :] == slot).astype(F32).reshape(experts * cap, own_rows).astype(BF)

    squares = jnp.zeros((own_rows, 1), F32)
    for n in range(0, weight.shape[1], block):
        stream = (res_ref[:, n : n + block].astype(F32) + total_ref[:, n : n + block]).astype(BF)
        stream_out[:, n : n + block] = stream
        wide = stream.astype(F32)
        squares = squares + jnp.sum(wide * wide, axis=1, keepdims=True)
    scale = lax.rsqrt(squares / weight.shape[1] + NORM_EPS)
    for n in range(0, weight.shape[1], block):
        cols = slice(n, n + block)
        normed = (stream_out[:, cols].astype(F32) * scale * gain_ref[:, cols]).astype(BF)
        normed_out[:, cols] = normed
        sent = jnp.dot(chosen, normed, preferred_element_type=F32).astype(BF)
        send_out[:, :, cols] = sent.reshape(experts, cap, block)


def post(info, parts, weights, residual, gain, ids_t, experts, cap):
    rows, width = residual.shape
    vmem = pl.BlockSpec(memory_space=pltpu.VMEM)
    return pl.pallas_call(
        functools.partial(post_kernel, tps=len(weights)),
        in_specs=[pl.BlockSpec(memory_space=pltpu.SMEM), vmem]
        + [pl.BlockSpec(memory_space=pltpu.HBM)] * len(weights)
        + [vmem] * 3,
        out_specs=[vmem] * 3,
        scratch_shapes=[
            pltpu.VMEM((rows, width), F32),
            pltpu.VMEM((width, width), BF),
            pltpu.VMEM((2 * len(weights), rows, HEAD_DIM), F32),
            pltpu.SemaphoreType.DMA((len(weights),)),
        ],
        out_shape=[
            jax.ShapeDtypeStruct((rows, width), BF),
            jax.ShapeDtypeStruct((rows, width), BF),
            jax.ShapeDtypeStruct((experts, cap, width), BF),
        ],
        compiler_params=pltpu.CompilerParams(vmem_limit_bytes=40 * 1024 * 1024),
        name="post",
    )(info, parts, *weights, residual, gain, ids_t)


def expert_kernel(x_ref, gate_ref, up_ref, down_ref, out_ref):
    peers, cap, width = x_ref.shape
    x = x_ref[...].reshape(peers * cap, width)
    gate = jnp.dot(x, gate_ref[0], preferred_element_type=F32)
    up = jnp.dot(x, up_ref[0], preferred_element_type=F32)
    hidden = (gate / (1.0 + jnp.exp(-gate)) * up).astype(BF)
    out = jnp.dot(hidden, down_ref[0], preferred_element_type=F32).astype(BF)
    out_ref[...] = out.reshape(peers, cap, width)


def expert(arrived, gate, up, down, steps=2):
    peers, cap, width = arrived.shape
    rows = pl.BlockSpec((peers // steps, cap, width), lambda g: (g, 0, 0))
    whole = lambda g: (0, 0, 0)
    return pl.pallas_call(
        expert_kernel,
        grid=(steps,),
        in_specs=[
            rows,
            pl.BlockSpec(gate.shape, whole),
            pl.BlockSpec(up.shape, whole),
            pl.BlockSpec(down.shape, whole),
        ],
        out_specs=rows,
        out_shape=pltpu.HBM(arrived.shape, BF),
        compiler_params=pltpu.CompilerParams(
            dimension_semantics=("arbitrary",), vmem_limit_bytes=40 * 1024 * 1024
        ),
        name="expert",
    )(arrived, gate, up, down)


def mix_kernel(ids_ref, route_ref, mix, *, cap):
    rows = ids_ref.shape[0]
    slots = mix.shape[1]
    experts = slots // cap
    route = route_ref[...]
    gates = route / jnp.sum(route, axis=1, keepdims=True) * ROUTED_SCALE
    expert = lax.broadcasted_iota(jnp.int32, (rows, experts), 1)
    named = jnp.zeros((rows, experts), F32)
    gate = jnp.zeros((rows, experts), F32)
    for k in range(TOPK):
        here = ids_ref[:, k : k + 1] == expert
        named = jnp.where(here, 1.0, named)
        gate = jnp.where(here, gates[:, k : k + 1], gate)
    earlier = (
        lax.broadcasted_iota(jnp.int32, (rows, rows), 1)
        < lax.broadcasted_iota(jnp.int32, (rows, rows), 0)
    ).astype(BF)
    rank = jnp.dot(earlier, named.astype(BF), preferred_element_type=F32)
    rank = jnp.where(named > 0.5, rank, 128.0)
    high = gate.astype(BF)
    low = (gate - high.astype(F32)).astype(BF)
    slot = lax.broadcasted_iota(jnp.int32, (experts, slots), 1)
    first = lax.broadcasted_iota(jnp.int32, (experts, slots), 0) * cap
    spread = ((slot >= first) & (slot < first + cap)).astype(BF)
    stacked = jnp.concatenate([rank.astype(BF), high, low], axis=0)
    wide = jnp.dot(stacked, spread, preferred_element_type=F32)
    place = (lax.broadcasted_iota(jnp.int32, (rows, slots), 1) % cap).astype(F32)
    chosen = wide[:rows] == place
    mix[:rows] = jnp.where(chosen, wide[rows : 2 * rows], 0.0).astype(BF)
    mix[rows:] = jnp.where(chosen, wide[2 * rows :], 0.0).astype(BF)


def mixing(ids, route, experts, cap):
    return pl.pallas_call(
        functools.partial(mix_kernel, cap=cap),
        out_shape=jax.ShapeDtypeStruct((2 * ids.shape[0], experts * cap), BF),
        name="mixing",
    )(ids, route)


def finish_kernel(res_ref, base_ref, mix_ref, out_ref):
    rows = base_ref.shape[0]
    experts, cap, block = res_ref.shape
    results = res_ref[...].reshape(experts * cap, block)
    routed = jnp.dot(mix_ref[...], results, preferred_element_type=F32)
    out_ref[...] = (base_ref[...] + routed[:rows] + routed[rows:]).astype(BF)


def finish(results, base, mix, block=1024):
    experts, cap, width = results.shape
    rows = base.shape[0]
    tiled = pl.BlockSpec((rows, block), lambda g: (0, g))
    return pl.pallas_call(
        finish_kernel,
        grid=(width // block,),
        in_specs=[
            pl.BlockSpec((experts, cap, block), lambda g: (0, 0, g)),
            tiled,
            pl.BlockSpec(mix.shape, lambda g: (0, 0)),
        ],
        out_specs=tiled,
        out_shape=jax.ShapeDtypeStruct(base.shape, BF),
        compiler_params=pltpu.CompilerParams(dimension_semantics=("arbitrary",)),
        name="finish",
    )(results, base, mix)


def local(
    residual,
    queries,
    key_rows,
    value_rows,
    forget_sums,
    out_weight,
    norm_gain,
    expert_ids,
    route_weights,
    expert_gate,
    expert_up,
    expert_down,
    shared_gate,
    shared_up,
    shared_down,
):
    z_count = lax.axis_size("z")
    y_count = lax.axis_size("y")
    z = lax.axis_index("z")
    y = lax.axis_index("y")
    rows = queries.shape[0]
    experts = z_count * y_count * 2
    cap = 2 * residual.shape[0] * TOPK // experts

    tps = lax.axis_size("tp")
    core = lax.axis_index("c")
    info = jnp.stack([2 * y * rows, z, lax.axis_index("tp"), core]).astype(jnp.int32)
    f_t = forget_sums.T
    mine, other = pack_keys(info, key_rows, value_rows, f_t)
    theirs = lax.ppermute(other, "c", [(0, 1), (1, 0)])
    own = jnp.stack([mine, theirs])
    up_ring = [(i, (i + 1) % z_count) for i in range(z_count)]
    down_ring = [(i, (i - 1) % z_count) for i in range(z_count)]
    q_send = pack_queries(queries, f_t, other, y_count)
    q_all = lax.all_to_all(q_send, ("y", "c"), split_axis=0, concat_axis=0)
    turn = [(i, (i + 1) % tps) for i in range(tps)]
    turn += [(tps + i, tps + (i - 1) % tps) for i in range(tps)]
    w_near = lax.ppermute(out_weight, ("c", "tp"), turn)

    def up(block):
        return lax.ppermute(block, "z", up_ring)

    def down(block):
        return lax.ppermute(block, "z", down_ring)

    up1, down1 = up(own), down(own)
    up2, down2 = up(up1), down(down1)
    state = attend(info, q_all, [own, up1, down1], (0, 1, -1), z_count, None, False)
    state, up2, down2, w_near = lax.optimization_barrier((state, up2, down2, w_near))
    up3, down3 = up(up2), down(down2)
    w_far = lax.ppermute(w_near, ("c", "tp"), turn)
    state = attend(info, q_all, [up2, down2], (2, -2), z_count, state, False)
    state, up3, down3 = lax.optimization_barrier((state, up3, down3))
    up4 = up(up3)
    w_other = lax.ppermute(w_near, "c", [(0, 1), (1, 0)])
    state = attend(info, q_all, [up3, down3], (3, -3), z_count, state, False)
    sent = attend(info, q_all, [up4], (4,), z_count, state, True)
    parts = lax.all_to_all(sent, ("y", "c", "tp"), split_axis=0, concat_axis=0)
    weights = [out_weight, w_near, w_other, w_far]
    stream, normed, outgoing = post(
        info,
        parts,
        weights,
        residual,
        norm_gain[None, :],
        expert_ids.T,
        experts,
        cap,
    )
    arrived = lax.all_to_all(outgoing, ("z", "y", "c"), split_axis=0, concat_axis=0)
    shared_hidden = (
        jax.nn.silu(jnp.dot(normed, shared_gate, preferred_element_type=F32))
        * jnp.dot(normed, shared_up, preferred_element_type=F32)
    ).astype(BF)
    base = stream.astype(F32) + jnp.dot(shared_hidden, shared_down, preferred_element_type=F32)
    processed = expert(arrived, expert_gate, expert_up, expert_down)
    returned = lax.all_to_all(
        processed, ("z", "y", "c"), split_axis=0, concat_axis=0
    )
    mix = mixing(expert_ids, route_weights, experts, cap)
    return finish(returned, base, mix)


def solution(mesh):
    sp = mesh.shape["sp"]
    tp = mesh.shape["tp"]
    grid = Mesh(mesh.devices.reshape(8, sp // 16, 2, tp), ("z", "y", "c", "tp"))
    seq = ("z", "y", "c")
    in_specs = (
        P((*seq, "tp"), None),
        P(seq, "tp"),
        P(seq, "tp"),
        P(seq, "tp"),
        P(seq, "tp"),
        P("tp", None),
        P(),
        P((*seq, "tp"), None),
        P((*seq, "tp"), None),
        P(seq, None, None),
        P(seq, None, None),
        P(seq, None, None),
        P(),
        P(),
        P(),
    )
    out_specs = P((*seq, "tp"), None)

    return jax.shard_map(local, mesh=grid, in_specs=in_specs, out_specs=out_specs, check_vma=False)
```

```python
import functools
import math

import jax
import jax.numpy as jnp
from jax import lax
from jax.experimental import pallas as pl
from jax.experimental.pallas import tpu as pltpu
from jax.sharding import Mesh, PartitionSpec as P

HEAD_DIM = 128
TOPK = 4
ROUTED_SCALE = 2.5
NORM_EPS = 1e-06
LOG2E = math.log2(math.e)
SCORE2 = HEAD_DIM**-0.5 * LOG2E
LOW = -1e30
TAIL = 8

BF = jnp.bfloat16
F32 = jnp.float32


def pieces(row):
    high = row.astype(BF)
    rest = row - high.astype(F32)
    mid = rest.astype(BF)
    low = (rest - mid.astype(F32)).astype(BF)
    return [high.astype(F32), mid.astype(F32), low.astype(F32)]


def tail_block(rows, width):
    parts = [piece for row in rows for piece in pieces(row)]
    parts.append(jnp.zeros((TAIL - len(parts), width), F32))
    return jnp.concatenate(parts, axis=0).astype(BF)


def row_of(tail, j):
    return tail[3 * j : 3 * j + 1] + tail[3 * j + 1 : 3 * j + 2] + tail[3 * j + 2 : 3 * j + 3]


def pack_keys_kernel(info, k_ref, v_ref, f_ref, mine, other):
    rows = k_ref.shape[0]
    for out, c in ((mine, info[3]), (other, 1 - info[3])):
        cols = pl.ds(pl.multiple_of(c * HEAD_DIM, HEAD_DIM), HEAD_DIM)
        out[:rows, :HEAD_DIM] = k_ref[:, cols]
        out[:rows, HEAD_DIM:] = v_ref[:, cols]
        out[rows:, :] = tail_block([f_ref[pl.ds(2 * c + j, 1), :] for j in range(2)], rows)


def pack_queries_kernel(q_ref, f_ref, _, out):
    rows = q_ref.shape[0]
    for c in range(2):
        tail = tail_block([f_ref[2 * c : 2 * c + 1, :], f_ref[2 * c + 1 : 2 * c + 2, :]], rows)
        part = q_ref[:, c * 2 * HEAD_DIM : (c + 1) * 2 * HEAD_DIM]
        for y in range(out.shape[0] // 2):
            out[2 * y + c, :rows, :] = part
            out[2 * y + c, rows:, :] = tail


def pack_keys(info, k, v, f_t):
    shape = (k.shape[0] + TAIL, 2 * HEAD_DIM)
    vmem = pl.BlockSpec(memory_space=pltpu.VMEM)
    return pl.pallas_call(
        pack_keys_kernel,
        in_specs=[pl.BlockSpec(memory_space=pltpu.SMEM)] + [vmem] * 3,
        out_shape=(pltpu.HBM(shape, BF), pltpu.HBM(shape, BF)),
        name="pack_keys",
    )(info, k, v, f_t)


def pack_queries(q, f_t, after, ys):
    return pl.pallas_call(
        pack_queries_kernel,
        in_specs=[pl.BlockSpec(), pl.BlockSpec(), pl.BlockSpec(memory_space=pl.ANY)],
        out_shape=pltpu.HBM((2 * ys, q.shape[0] + TAIL, 2 * HEAD_DIM), BF),
        name="pack_queries",
    )(q, f_t, after)


def attend_kernel(info, *refs, steps, z_count, first, last, tiles, rows):
    blocks, own = len(steps), 0 in steps
    q_ref = refs[0]
    kv_refs = refs[1 : 1 + blocks]
    at = 1 + blocks
    if not first:
        acc_in, stat_in = refs[at], refs[at + 1]
        at += 2
    if last:
        (o_out,) = refs[at : at + 1]
    else:
        acc_out, stat_out = refs[at : at + 2]
    first_tail = q_ref[0, rows:, :].astype(F32)
    keys, values, biases = [], [], []
    ones = jnp.ones((rows, HEAD_DIM), BF)
    for b, s in enumerate(steps):
        valid = info[1] >= s if s >= 0 else info[1] - s >= z_count
        for c in range(2):
            keys.append(kv_refs[b].at[c, pl.ds(0, rows), pl.ds(0, HEAD_DIM)])
            values.append(kv_refs[b].at[c, pl.ds(0, rows), pl.ds(HEAD_DIM, HEAD_DIM)])
            tail = kv_refs[b][c, rows:, :].astype(F32)
            pair = []
            for j in range(2):
                bias = (row_of(first_tail, j)[:, :1] - row_of(tail, j)) * LOG2E
                pair.append(jnp.where(valid, bias, -jnp.inf))
            biases.append(pair)

    def score_tiles(i):
        both = jnp.concatenate(
            [q_ref[i, pl.ds(0, rows), pl.ds(j * HEAD_DIM, HEAD_DIM)] for j in range(2)], axis=0
        )
        found = [[], []]
        for u in range(2 * blocks):
            raw = lax.dot_general(
                both, keys[u][...], (((1,), (1,)), ((), ())), preferred_element_type=F32
            )
            for j in range(2):
                score = raw[j * rows : (j + 1) * rows] * SCORE2 + biases[u][j]
                if own and u < 2:
                    q_pos = i * rows + lax.broadcasted_iota(
                        jnp.int32, (rows, rows), 0
                    )
                    k_pos = info[0] + (u ^ info[3]) * rows + lax.broadcasted_iota(jnp.int32, (rows, rows), 1)
                    score = jnp.where(q_pos >= k_pos, score, -jnp.inf)
                found[j].append(score)
        return found

    def absorb(i, scores):
        maxes, olds = [], []
        for j in range(2):
            top = scores[j][0]
            for score in scores[j][1:]:
                top = jnp.maximum(top, score)
            row_max = jnp.max(top, axis=1, keepdims=True)
            cols = pl.ds(j * HEAD_DIM, HEAD_DIM)
            old_max = jnp.full((rows, HEAD_DIM), LOW, F32) if first else stat_in[i, :, cols]
            olds.append(old_max)
            maxes.append(jnp.maximum(row_max, old_max))
        total = None
        wide = rows // HEAD_DIM
        for u in range(2 * blocks):
            weights = jnp.concatenate(
                [
                    jnp.exp2(scores[j][u] - jnp.concatenate([maxes[j]] * wide, axis=1)).astype(BF)
                    for j in range(2)
                ],
                axis=0,
            )
            value = jnp.concatenate([values[u][...], ones], axis=1)
            part = jnp.dot(weights, value, preferred_element_type=F32)
            total = part if total is None else total + part
        lse_rows = []
        for j in range(2):
            cols = pl.ds(j * HEAD_DIM, HEAD_DIM)
            weighted = total[j * rows : (j + 1) * rows, :HEAD_DIM]
            row_sum = total[j * rows : (j + 1) * rows, HEAD_DIM:]
            if not first:
                factor = jnp.exp2(olds[j] - maxes[j])
                sums = pl.ds((2 + j) * HEAD_DIM, HEAD_DIM)
                weighted = weighted + acc_in[i, :, cols] * factor
                row_sum = row_sum + acc_in[i, :, sums] * factor
            if last:
                some = row_sum > 0.0
                row_sum = jnp.where(some, row_sum, 1.0)
                mixed = weighted * (1.0 / row_sum)
                per = rows // 4
                for p in range(4):
                    o_out[4 * i + p, pl.ds(0, per), cols] = mixed[p * per : (p + 1) * per].astype(BF)
                lse = jnp.where(some, maxes[j] + jnp.log2(row_sum), LOW)
                flat = []
                eye = lax.broadcasted_iota(jnp.int32, (HEAD_DIM, HEAD_DIM), 0) == (
                    lax.broadcasted_iota(jnp.int32, (HEAD_DIM, HEAD_DIM), 1)
                )
                for at in range(0, rows, HEAD_DIM):
                    flat.append(
                        jnp.sum(jnp.where(eye, lse[at : at + HEAD_DIM], 0.0), axis=0, keepdims=True)
                    )
                lse_rows.append(jnp.concatenate(flat, axis=1))
            else:
                acc_out[i, :, cols] = weighted
                acc_out[i, :, pl.ds((2 + j) * HEAD_DIM, HEAD_DIM)] = row_sum
                stat_out[i, :, cols] = maxes[j]
        if last:
            tail = tail_block(lse_rows, rows)
            for p in range(4):
                o_out[4 * i + p, pl.ds(rows // 4, TAIL), :] = tail

    def some_tiles(step, _):
        pending = score_tiles(step * tiles)
        for n in range(tiles):
            i = step * tiles + n
            following = score_tiles(i + 1) if n + 1 < tiles else None
            absorb(i, pending)
            pending = following
        return 0

    lax.fori_loop(0, q_ref.shape[0] // tiles, some_tiles, 0)


def attend(info, q_all, kvs, steps, z_count, state, last, tiles=4):
    count, padded, width = q_all.shape
    rows = padded - TAIL
    first = state is None
    blocks = len(kvs)
    vmem = pl.BlockSpec(memory_space=pltpu.VMEM)
    operands = [q_all, *kvs]
    aliases = {}
    if not first:
        operands += list(state)
        if not last:
            aliases = {len(operands) - 1: 0, len(operands): 1}
    if last:
        out_shape = jax.ShapeDtypeStruct((4 * count, rows // 4 + TAIL, width), BF)
    else:
        out_shape = [
            jax.ShapeDtypeStruct((count, rows, 2 * width), F32),
            jax.ShapeDtypeStruct((count, rows, width), F32),
        ]
    scores = count * rows * 2 * blocks * 2 * rows
    return pl.pallas_call(
        functools.partial(
            attend_kernel, steps=steps, z_count=z_count, first=first, last=last, tiles=tiles, rows=rows
        ),
        in_specs=[pl.BlockSpec(memory_space=pltpu.SMEM)] + [vmem] * len(operands),
        out_specs=vmem if last else [vmem, vmem],
        out_shape=out_shape,
        input_output_aliases=aliases,
        cost_estimate=pl.CostEstimate(
            flops=scores * 768, transcendentals=scores, bytes_accessed=6_000_000
        ),
        compiler_params=pltpu.CompilerParams(vmem_limit_bytes=24 * 1024 * 1024),
    )(info, *operands)


def post_kernel(info, part_ref, *refs, tps):
    w_refs = refs[:tps]
    res_ref, gain_ref, ids_ref, stream_out, normed_out, send_out, total_ref, weight, share, sems = refs[tps:]
    sources = part_ref.shape[0]
    own_rows = res_ref.shape[0]
    width = part_ref.shape[2]
    groups = 2 * tps
    ys = sources // groups
    copies = []
    at = 0
    for n, w_ref in enumerate(w_refs):
        size = w_ref.shape[0]
        copies.append(pltpu.make_async_copy(w_ref, weight.at[pl.ds(at, size)], sems.at[n]))
        copies[-1].start()
        at += size

    pick = lax.broadcasted_iota(jnp.int32, (own_rows, width), 1) == (
        info[2] * own_rows + lax.broadcasted_iota(jnp.int32, (own_rows, width), 0)
    )
    tails = part_ref[:, own_rows:, :].reshape(sources * TAIL, width)
    pieces_t = lax.dot_general(
        pick.astype(F32).astype(BF), tails, (((1,), (1,)), ((), ())), preferred_element_type=F32
    )
    last = pieces_t.shape[1]
    lses = pieces_t + pltpu.roll(pieces_t, last - 1, 1) + pltpu.roll(pieces_t, last - 2, 1)
    span = last // ys
    lses = [lses[:, y * span : (y + 1) * span] for y in range(ys)]
    top = lses[0]
    for one in lses[1:]:
        top = jnp.maximum(top, one)
    shares = [jnp.exp2(one - top) for one in lses]
    total = shares[0]
    for one in shares[1:]:
        total = total + one
    inverse = 1.0 / total
    shares = [one * inverse for one in shares]
    spare = jnp.zeros((own_rows, HEAD_DIM - 2 * ys), F32)
    for index in range(groups):
        columns = [
            shares[y][:, TAIL * index + 3 * j : TAIL * index + 3 * j + 1]
            for y in range(ys)
            for j in range(2)
        ]
        share[index] = jnp.concatenate([*columns, spare], axis=1)
    near = 2 * info[3] - 1
    turns = [(info[2] + turn + tps) % tps for turn in (0, near, -near, 2)]
    block = 2 * width
    quarter = weight.shape[0] // tps
    for s, tp in enumerate(turns):
        merged = []
        for core in range(2):
            index = core * tps + tp
            for j in range(2):
                mixed = None
                for y in range(ys):
                    part = part_ref[
                        y * groups + index, pl.ds(0, own_rows), pl.ds(j * HEAD_DIM, HEAD_DIM)
                    ].astype(F32) * share[index, :, y * 2 + j : y * 2 + j + 1]
                    mixed = part if mixed is None else mixed + part
                merged.append(mixed.astype(BF))
        attended = jnp.concatenate(merged, axis=1)
        copies[s].wait()
        for n in range(0, weight.shape[1], block):
            product = jnp.dot(
                attended,
                weight[s * quarter : (s + 1) * quarter, n : n + block],
                preferred_element_type=F32,
            )
            total_ref[:, n : n + block] = product if s == 0 else total_ref[:, n : n + block] + product

    experts = send_out.shape[0]
    cap = send_out.shape[1]
    expert = lax.broadcasted_iota(jnp.int32, (experts, own_rows), 0)
    named = jnp.zeros((experts, own_rows), F32)
    for k in range(TOPK):
        named = jnp.where(ids_ref[k : k + 1, :] == expert, 1.0, named)
    earlier = (
        lax.broadcasted_iota(jnp.int32, (own_rows, own_rows), 0)
        < lax.broadcasted_iota(jnp.int32, (own_rows, own_rows), 1)
    ).astype(BF)
    rank = jnp.dot(named.astype(BF), earlier, preferred_element_type=F32)
    rank = jnp.where(named > 0.5, rank, -1.0)
    slot = lax.broadcasted_iota(jnp.int32, (experts, cap, own_rows), 1).astype(F32)
    chosen = (rank[:, None, :] == slot).astype(F32).reshape(experts * cap, own_rows).astype(BF)

    squares = jnp.zeros((own_rows, 1), F32)
    for n in range(0, weight.shape[1], block):
        stream = (res_ref[:, n : n + block].astype(F32) + total_ref[:, n : n + block]).astype(BF)
        stream_out[:, n : n + block] = stream
        wide = stream.astype(F32)
        squares = squares + jnp.sum(wide * wide, axis=1, keepdims=True)
    scale = lax.rsqrt(squares / weight.shape[1] + NORM_EPS)
    for n in range(0, weight.shape[1], block):
        cols = slice(n, n + block)
        normed = (stream_out[:, cols].astype(F32) * scale * gain_ref[:, cols]).astype(BF)
        normed_out[:, cols] = normed
        sent = jnp.dot(chosen, normed, preferred_element_type=F32).astype(BF)
        send_out[:, :, cols] = sent.reshape(experts, cap, block)


def post(info, parts, weights, residual, gain, ids_t, experts, cap):
    rows, width = residual.shape
    vmem = pl.BlockSpec(memory_space=pltpu.VMEM)
    return pl.pallas_call(
        functools.partial(post_kernel, tps=len(weights)),
        in_specs=[pl.BlockSpec(memory_space=pltpu.SMEM), vmem]
        + [pl.BlockSpec(memory_space=pltpu.HBM)] * len(weights)
        + [vmem] * 3,
        out_specs=[vmem] * 3,
        scratch_shapes=[
            pltpu.VMEM((rows, width), F32),
            pltpu.VMEM((width, width), BF),
            pltpu.VMEM((2 * len(weights), rows, HEAD_DIM), F32),
            pltpu.SemaphoreType.DMA((len(weights),)),
        ],
        out_shape=[
            jax.ShapeDtypeStruct((rows, width), BF),
            jax.ShapeDtypeStruct((rows, width), BF),
            jax.ShapeDtypeStruct((experts, cap, width), BF),
        ],
        compiler_params=pltpu.CompilerParams(vmem_limit_bytes=40 * 1024 * 1024),
        name="post",
    )(info, parts, *weights, residual, gain, ids_t)


def expert_kernel(x_ref, gate_ref, up_ref, down_ref, out_ref, staged, sems, *, steps):
    peers, cap, width = x_ref.shape
    part = peers // steps
    copies = []
    for n in range(steps):
        rows = pl.ds(n * part, part)
        x = x_ref[rows].reshape(part * cap, width)
        gate = jnp.dot(x, gate_ref[0], preferred_element_type=F32)
        up = jnp.dot(x, up_ref[0], preferred_element_type=F32)
        hidden = (gate / (1.0 + jnp.exp(-gate)) * up).astype(BF)
        out = jnp.dot(hidden, down_ref[0], preferred_element_type=F32).astype(BF)
        staged[rows] = out.reshape(part, cap, width)
        copies.append(pltpu.make_async_copy(staged.at[rows], out_ref.at[rows], sems.at[n]))
        copies[-1].start()
    for copy in copies:
        copy.wait()


def expert(arrived, gate, up, down, steps=2):
    vmem = pl.BlockSpec(memory_space=pltpu.VMEM)
    return pl.pallas_call(
        functools.partial(expert_kernel, steps=steps),
        in_specs=[vmem] * 4,
        out_specs=pl.BlockSpec(memory_space=pltpu.HBM),
        out_shape=pltpu.HBM(arrived.shape, BF),
        scratch_shapes=[pltpu.VMEM(arrived.shape, BF), pltpu.SemaphoreType.DMA((steps,))],
        compiler_params=pltpu.CompilerParams(vmem_limit_bytes=32 * 1024 * 1024),
        name="expert",
    )(arrived, gate, up, down)


def mix_kernel(ids_ref, route_ref, mix, *, cap):
    rows = ids_ref.shape[0]
    slots = mix.shape[1]
    experts = slots // cap
    route = route_ref[...]
    gates = route / jnp.sum(route, axis=1, keepdims=True) * ROUTED_SCALE
    expert = lax.broadcasted_iota(jnp.int32, (rows, experts), 1)
    named = jnp.zeros((rows, experts), F32)
    gate = jnp.zeros((rows, experts), F32)
    for k in range(TOPK):
        here = ids_ref[:, k : k + 1] == expert
        named = jnp.where(here, 1.0, named)
        gate = jnp.where(here, gates[:, k : k + 1], gate)
    earlier = (
        lax.broadcasted_iota(jnp.int32, (rows, rows), 1)
        < lax.broadcasted_iota(jnp.int32, (rows, rows), 0)
    ).astype(BF)
    rank = jnp.dot(earlier, named.astype(BF), preferred_element_type=F32)
    rank = jnp.where(named > 0.5, rank, 128.0)
    high = gate.astype(BF)
    low = (gate - high.astype(F32)).astype(BF)
    slot = lax.broadcasted_iota(jnp.int32, (experts, slots), 1)
    first = lax.broadcasted_iota(jnp.int32, (experts, slots), 0) * cap
    spread = ((slot >= first) & (slot < first + cap)).astype(BF)
    stacked = jnp.concatenate([rank.astype(BF), high, low], axis=0)
    wide = jnp.dot(stacked, spread, preferred_element_type=F32)
    place = (lax.broadcasted_iota(jnp.int32, (rows, slots), 1) % cap).astype(F32)
    chosen = wide[:rows] == place
    mix[:rows] = jnp.where(chosen, wide[rows : 2 * rows], 0.0).astype(BF)
    mix[rows:] = jnp.where(chosen, wide[2 * rows :], 0.0).astype(BF)


def mixing(ids, route, experts, cap):
    return pl.pallas_call(
        functools.partial(mix_kernel, cap=cap),
        out_shape=jax.ShapeDtypeStruct((2 * ids.shape[0], experts * cap), BF),
        name="mixing",
    )(ids, route)


def finish_kernel(res_ref, base_ref, mix_ref, out_ref):
    rows = base_ref.shape[0]
    experts, cap, block = res_ref.shape
    results = res_ref[...].reshape(experts * cap, block)
    routed = jnp.dot(mix_ref[...], results, preferred_element_type=F32)
    out_ref[...] = (base_ref[...] + routed[:rows] + routed[rows:]).astype(BF)


def finish(results, base, mix, block=1024):
    experts, cap, width = results.shape
    rows = base.shape[0]
    tiled = pl.BlockSpec((rows, block), lambda g: (0, g))
    return pl.pallas_call(
        finish_kernel,
        grid=(width // block,),
        in_specs=[
            pl.BlockSpec((experts, cap, block), lambda g: (0, 0, g)),
            tiled,
            pl.BlockSpec(mix.shape, lambda g: (0, 0)),
        ],
        out_specs=tiled,
        out_shape=jax.ShapeDtypeStruct(base.shape, BF),
        compiler_params=pltpu.CompilerParams(dimension_semantics=("arbitrary",)),
        name="finish",
    )(results, base, mix)


def local(
    residual,
    queries,
    key_rows,
    value_rows,
    forget_sums,
    out_weight,
    norm_gain,
    expert_ids,
    route_weights,
    expert_gate,
    expert_up,
    expert_down,
    shared_gate,
    shared_up,
    shared_down,
):
    z_count = lax.axis_size("z")
    y_count = lax.axis_size("y")
    z = lax.axis_index("z")
    y = lax.axis_index("y")
    rows = queries.shape[0]
    experts = z_count * y_count * 2
    cap = 2 * residual.shape[0] * TOPK // experts

    tps = lax.axis_size("tp")
    core = lax.axis_index("c")
    info = jnp.stack([2 * y * rows, z, lax.axis_index("tp"), core]).astype(jnp.int32)
    f_t = forget_sums.T
    mine, other = pack_keys(info, key_rows, value_rows, f_t)
    theirs = lax.ppermute(other, "c", [(0, 1), (1, 0)])
    own = jnp.stack([mine, theirs])
    up_ring = [(i, (i + 1) % z_count) for i in range(z_count)]
    down_ring = [(i, (i - 1) % z_count) for i in range(z_count)]
    q_send = pack_queries(queries, f_t, other, y_count)
    q_all = lax.all_to_all(q_send, ("y", "c"), split_axis=0, concat_axis=0)
    turn = [(i, (i + 1) % tps) for i in range(tps)]
    turn += [(tps + i, tps + (i - 1) % tps) for i in range(tps)]
    w_near = lax.ppermute(out_weight, ("c", "tp"), turn)

    def up(block):
        return lax.ppermute(block, "z", up_ring)

    def down(block):
        return lax.ppermute(block, "z", down_ring)

    up1, down1 = up(own), down(own)
    up2, down2 = up(up1), down(down1)
    state = attend(info, q_all, [own, up1, down1], (0, 1, -1), z_count, None, False)
    state, up2, down2, w_near = lax.optimization_barrier((state, up2, down2, w_near))
    up3, down3 = up(up2), down(down2)
    w_far = lax.ppermute(w_near, ("c", "tp"), turn)
    state = attend(info, q_all, [up2, down2], (2, -2), z_count, state, False)
    state, up3, down3 = lax.optimization_barrier((state, up3, down3))
    up4 = up(up3)
    w_other = lax.ppermute(w_near, "c", [(0, 1), (1, 0)])
    state = attend(info, q_all, [up3, down3], (3, -3), z_count, state, False)
    sent = attend(info, q_all, [up4], (4,), z_count, state, True, tiles=8)
    parts = lax.all_to_all(sent, ("y", "c", "tp"), split_axis=0, concat_axis=0)
    weights = [out_weight, w_near, w_other, w_far]
    stream, normed, outgoing = post(
        info,
        parts,
        weights,
        residual,
        norm_gain[None, :],
        expert_ids.T,
        experts,
        cap,
    )
    arrived = lax.all_to_all(outgoing, ("z", "y", "c"), split_axis=0, concat_axis=0)
    shared_hidden = (
        jax.nn.silu(jnp.dot(normed, shared_gate, preferred_element_type=F32))
        * jnp.dot(normed, shared_up, preferred_element_type=F32)
    ).astype(BF)
    base = stream.astype(F32) + jnp.dot(shared_hidden, shared_down, preferred_element_type=F32)
    processed = expert(arrived, expert_gate, expert_up, expert_down)
    returned = lax.all_to_all(
        processed, ("z", "y", "c"), split_axis=0, concat_axis=0
    )
    mix = mixing(expert_ids, route_weights, experts, cap)
    return finish(returned, base, mix)


def solution(mesh):
    sp = mesh.shape["sp"]
    tp = mesh.shape["tp"]
    grid = Mesh(mesh.devices.reshape(8, sp // 16, 2, tp), ("z", "y", "c", "tp"))
    seq = ("z", "y", "c")
    in_specs = (
        P((*seq, "tp"), None),
        P(seq, "tp"),
        P(seq, "tp"),
        P(seq, "tp"),
        P(seq, "tp"),
        P("tp", None),
        P(),
        P((*seq, "tp"), None),
        P((*seq, "tp"), None),
        P(seq, None, None),
        P(seq, None, None),
        P(seq, None, None),
        P(),
        P(),
        P(),
    )
    out_specs = P((*seq, "tp"), None)

    return jax.shard_map(local, mesh=grid, in_specs=in_specs, out_specs=out_specs, check_vma=False)
```
